32 devices in a mesh: sp: 8 (over z, x), tp: 4 (over y, core).
Axes of the slice: x: 2, y: 2, z: 4, core: 2. Of those that a mesh axis runs over, the one named last changes fastest.
Arguments:
- tokens: bfloat16 [3072, 2048], P('sp', 'tp'), may hold values from -6 to 6
- ret_query: bfloat16 [2048, 1024], P(None, 'tp'), may hold values from -0.125 to 0.125
- ret_key: bfloat16 [2048, 1024], P(None, 'tp'), may hold values from -0.125 to 0.125
- ret_value: bfloat16 [2048, 1024], P(None, 'tp'), may hold values from -0.125 to 0.125
- stick_query: bfloat16 [2048, 1024], P(None, 'tp'), may hold values from -0.125 to 0.125
- stick_key: bfloat16 [2048, 1024], P(None, 'tp'), may hold values from -0.125 to 0.125
- stick_value: bfloat16 [2048, 1024], P(None, 'tp'), may hold values from -0.125 to 0.125
- log_decay: float32 [3072, 8], P('sp', 'tp'), may hold values from -1.2 to 0
- stick_bias: float32 [8], P('tp'), may hold values from -13 to -5
- out_ret: bfloat16 [1024, 2048], P('tp'), may hold values from -0.125 to 0.125
- out_stick: bfloat16 [1024, 2048], P('tp'), may hold values from -0.125 to 0.125
Outputs:
- mixed: bfloat16 [3072, 2048], P('sp', 'tp')
The draws below stay inside these ranges and needn't reach their ends.
All inputs are finite; a program needn't handle non-finite values.
Results may differ from the reference program's by a relative error of at most 0.019.
Values may be sent and summed in bfloat16 or wider, within the bound.
A program may use at most 64 MiB of HBM per device.

```python
import jax
import jax.numpy as jnp
from jax import lax

D = 2048
HEAD_DIM = 128
RET_HEADS = 8
SB_HEADS = 8
TOK_DEV = 384
TOKENS = 3072


def draw_log_decay(key, part):
    streams = jax.random.split(key, 7)
    slow_share = 0.5
    base_rate = jax.random.uniform(streams[0], (RET_HEADS,), jnp.float32, 0.2, 0.5)
    slow_heads = jax.random.bernoulli(streams[1], slow_share, (RET_HEADS,))
    fast_rate = jax.random.uniform(streams[2], (RET_HEADS,), jnp.float32, 1.0 / 60.0, 1.0 / 30.0)
    head_decay_rate = jnp.where(slow_heads, base_rate / TOKENS, fast_rate)
    block_count = TOKENS // TOK_DEV
    block_multiplier = jnp.exp(jax.random.uniform(streams[3], (block_count, RET_HEADS), jnp.float32, -0.69, 0.69))
    block_multiplier = jnp.repeat(block_multiplier, TOK_DEV, axis=0)
    jaggedness = jnp.exp(jax.random.uniform(streams[4], (TOKENS, RET_HEADS), jnp.float32, -0.5, 0.47))
    location_list = jax.random.randint(streams[5], (2, RET_HEADS), 0, TOKENS)
    loss_values = jax.random.uniform(streams[6], (2, RET_HEADS), jnp.float32, 0.2, 0.4)
    row_position_index = jnp.arange(TOKENS, dtype=jnp.int32)[:, None]
    spike_groups = jnp.where(row_position_index == location_list[0][None, :], jnp.log(1.0 - loss_values[0])[None, :], 0.0)
    spike_groups = spike_groups + jnp.where(row_position_index == location_list[1][None, :], jnp.log(1.0 - loss_values[1])[None, :], 0.0)
    return (-head_decay_rate[None, :] * block_multiplier * jaggedness + spike_groups).astype(jnp.float32)


def draw_stick_bias(key, part):
    return jax.random.uniform(key, (SB_HEADS,), jnp.float32, -13.0, -5.0)


def block_levels(own_key, shape, pieces, smallest, high):
    def one(position, parts):
        draws = jax.random.uniform(jax.random.fold_in(jax.random.fold_in(own_key, 6), position), (parts,), jnp.float32, smallest / len(pieces), high / len(pieces))
        return jnp.repeat(jnp.exp(draws), shape[position] // parts).reshape((-1,) + (1,) * (len(shape) - position - 1))

    loudness = one(*pieces[0])
    for cut in pieces[1:]:
        loudness = loudness * one(*cut)
    return loudness


def scatter_about(key, extent, scale, bound, shards=(), kind=jnp.bfloat16):
    loudness = block_levels(key, extent, shards, -0.22, 0.18) if shards else 1.0
    entries = jax.random.normal(key, extent, jnp.float32) * scale * loudness
    return jnp.minimum(jnp.maximum(entries, -bound), bound).astype(kind)


def setup_inputs(seed: int = 0) -> dict:
    seeds = jax.random.split(jax.random.key(seed), 12)
    tokens = scatter_about(seeds[0], (TOKENS, D), 1.0, 6.0, ((0, 8), (1, 4)))
    ret_query = scatter_about(seeds[1], (D, RET_HEADS * HEAD_DIM), D ** -0.5, 0.125, ((1, 4),))
    ret_key = scatter_about(seeds[2], (D, RET_HEADS * HEAD_DIM), D ** -0.5, 0.125, ((1, 4),))
    ret_value = scatter_about(seeds[3], (D, RET_HEADS * HEAD_DIM), D ** -0.5, 0.125, ((1, 4),))
    stick_query = scatter_about(seeds[4], (D, SB_HEADS * HEAD_DIM), D ** -0.5, 0.125, ((1, 4),))
    stick_key = scatter_about(seeds[5], (D, SB_HEADS * HEAD_DIM), D ** -0.5, 0.125, ((1, 4),))
    stick_value = scatter_about(seeds[6], (D, SB_HEADS * HEAD_DIM), D ** -0.5, 0.125, ((1, 4),))
    log_decay = draw_log_decay(jax.random.fold_in(seeds[11], 71), 0)
    stick_bias = draw_stick_bias(jax.random.fold_in(seeds[11], 71), 0)
    out_ret = scatter_about(seeds[9], (RET_HEADS * HEAD_DIM, D), ((RET_HEADS + SB_HEADS) * HEAD_DIM) ** -0.5, 0.125, ((0, 4),))
    out_stick = scatter_about(seeds[10], (SB_HEADS * HEAD_DIM, D), ((RET_HEADS + SB_HEADS) * HEAD_DIM) ** -0.5, 0.125, ((0, 4),))
    return dict(tokens=tokens, ret_query=ret_query, ret_key=ret_key, ret_value=ret_value, stick_query=stick_query, stick_key=stick_key, stick_value=stick_value, log_decay=log_decay, stick_bias=stick_bias, out_ret=out_ret, out_stick=out_stick)


EPS = 1e-05
ROPE_BASE = 10000.0

def rounded(values):
    return lax.optimization_barrier(values.astype(jnp.bfloat16)).astype(jnp.float32)

def rotate(values, positions):
    half_width = values.shape[-1] // 2
    inverse = ROPE_BASE ** (-jnp.arange(half_width, dtype=jnp.float32) / half_width)
    angles = positions[:, None] * inverse[None, :]
    cosine = jnp.cos(angles)[:, None, :]
    sine_part = jnp.sin(angles)[:, None, :]
    first_half = values[..., :half_width]
    second_half = values[..., half_width:]
    return jnp.concatenate([first_half * cosine - second_half * sine_part, first_half * sine_part + second_half * cosine], axis=-1)

def head_norm(values):
    centred = values - lax.optimization_barrier(jnp.mean(values, axis=-1, keepdims=True))
    spread = lax.optimization_barrier(jnp.mean(centred * centred, axis=-1, keepdims=True))
    return centred * lax.rsqrt(spread + EPS)

def retention(query_rot, key_rot, value_rows, log_decay):
    blocks = TOKENS // TOK_DEV
    head_count = query_rot.shape[1]
    index_rows = jnp.arange(TOK_DEV, dtype=jnp.int32)
    lower = (index_rows[:, None] >= index_rows[None, :])[None]

    def split(values):
        return values.reshape((blocks, TOK_DEV) + values.shape[1:])

    def advance(state, block):
        query_block, key_block, value_block, decay_block = block
        cumulative = jnp.cumsum(decay_block, axis=0)
        final_decay = cumulative[-1]
        gaps = cumulative.T[:, :, None] - cumulative.T[:, None, :]
        decay = jnp.where(lower, jnp.exp(jnp.where(lower, gaps, 0.0)), 0.0)
        scores = jnp.einsum('thd,shd->hts', query_block.astype(jnp.float32), key_block.astype(jnp.float32))
        inner = rounded(scores * decay)
        local_part = jnp.einsum('hts,she->the', inner, value_block.astype(jnp.float32))
        carried = jnp.einsum('thd,hde->the', query_block.astype(jnp.float32), state, precision=lax.Precision.HIGHEST) * jnp.exp(cumulative)[:, :, None]
        weighted = rounded(key_block.astype(jnp.float32) * jnp.exp(final_decay[None, :] - cumulative)[:, :, None])
        fresh = jnp.einsum('shd,she->hde', weighted, value_block.astype(jnp.float32))
        state = jnp.exp(final_decay)[:, None, None] * state + fresh
        return (state, local_part + carried)
    start_state = jnp.zeros((head_count, HEAD_DIM, HEAD_DIM), jnp.float32)
    _, outputs = lax.scan(advance, start_state, (split(query_rot), split(key_rot), split(value_rows), split(log_decay)))
    return outputs.reshape(TOKENS, head_count, HEAD_DIM)

def stick_breaking(queries, keys, values, bias):
    blocks = TOKENS // TOK_DEV
    head_count = queries.shape[1]
    scale = HEAD_DIM ** (-0.5)
    keys_heads = jnp.transpose(keys, (1, 0, 2)).astype(jnp.float32)
    values_heads = jnp.transpose(values, (1, 0, 2)).astype(jnp.float32).reshape(head_count, blocks, TOK_DEV, HEAD_DIM)
    key_pos = jnp.arange(TOKENS, dtype=jnp.int32)

    def one_block(index):
        block_queries = lax.dynamic_slice_in_dim(queries, index * TOK_DEV, TOK_DEV, 0)
        query_heads = jnp.transpose(block_queries, (1, 0, 2)).astype(jnp.float32)
        query_pos = index * TOK_DEV + jnp.arange(TOK_DEV, dtype=jnp.int32)
        visible = (key_pos[None, :] < query_pos[:, None]).reshape(TOK_DEV, blocks, TOK_DEV)

        def one_head(query_h, key_h, value_h, bias_h):
            logits = (jnp.dot(query_h, key_h.T) * scale + bias_h).reshape(TOK_DEV, blocks, TOK_DEV)
            success = jax.nn.log_sigmoid(logits)
            failure = jnp.where(visible, success - logits, 0.0)
            suffix = lax.cumsum(failure, axis=2, reverse=True) - failure
            weights = rounded(jnp.where(visible, jnp.exp(success + suffix), 0.0))
            partial_value = jnp.einsum('tpk,pke->tpe', weights, value_h)
            totals = lax.optimization_barrier(jnp.sum(failure, axis=2))
            behind = lax.cumsum(totals, axis=1, reverse=True) - totals
            return lax.optimization_barrier(jnp.sum(jnp.exp(behind)[:, :, None] * partial_value, axis=1))
        return jax.vmap(one_head)(query_heads, keys_heads, values_heads, bias)
    outputs = lax.map(one_block, jnp.arange(blocks, dtype=jnp.int32))
    return jnp.transpose(outputs, (0, 2, 1, 3)).reshape(TOKENS, head_count, HEAD_DIM)

def reference(tokens, ret_query, ret_key, ret_value, stick_query, stick_key, stick_value, log_decay, stick_bias, out_ret, out_stick):

    def project(matrix):
        return jnp.dot(tokens, matrix, preferred_element_type=jnp.float32).astype(jnp.bfloat16).reshape(TOKENS, -1, HEAD_DIM)
    positions = jnp.arange(TOKENS, dtype=jnp.float32)
    query_rot = rotate(project(ret_query).astype(jnp.float32), positions).astype(jnp.bfloat16)
    key_rot = (rotate(project(ret_key).astype(jnp.float32), positions) * HEAD_DIM ** (-0.5)).astype(jnp.bfloat16)
    ret_out = head_norm(retention(query_rot, key_rot, project(ret_value), log_decay)).astype(jnp.bfloat16)
    stick_out = head_norm(stick_breaking(project(stick_query), project(stick_key), project(stick_value), stick_bias)).astype(jnp.bfloat16)
    mixed = jnp.dot(ret_out.reshape(TOKENS, -1), out_ret, preferred_element_type=jnp.float32)
    mixed = mixed + jnp.dot(stick_out.reshape(TOKENS, -1), out_stick, preferred_element_type=jnp.float32)
    return mixed.astype(jnp.bfloat16)
```

```python
import functools

import jax
import jax.numpy as jnp
import numpy as np
from jax import lax
from jax.experimental import pallas as pl
from jax.experimental.pallas import tpu as pltpu
from jax.sharding import PartitionSpec as P

HEAD_DIM = 128
EPS = 1e-05
ROPE_BASE = 10000.0
CORES = 2
CHUNK = 128
BIT = 64
TILE = 256
LOG2E = 1.4426950408889634
CLIP = 40.0
F32 = jnp.float32
BF16 = jnp.bfloat16


def row_width(shards):
    width = 1
    while (2 * width) ** 2 <= shards and shards % (2 * width) == 0:
        width *= 2
    return width


def head_norm(values):
    centred = values - jnp.mean(values, axis=-1, keepdims=True)
    spread = jnp.mean(centred * centred, axis=-1, keepdims=True)
    return centred * lax.rsqrt(spread + EPS)


def nt(a, b):
    return lax.dot_general(a, b, (((1,), (1,)), ((), ())), preferred_element_type=F32)


def dot(a, b):
    return jnp.dot(a, b, preferred_element_type=F32)


def kernel(
    shards,
    parts,
    tok,
    w_rq,
    w_rk,
    w_rv,
    w_sq,
    w_sk,
    w_sv,
    o_ret,
    o_stick,
    log_decay,
    inverse,
    bias,
    out,
    xs,
    wall,
    wo,
    acc,
    kv,
    sq,
    qrot,
    retv,
    local,
    tri,
    cumb,
    fresh,
    st_in,
    st_out,
    running,
    trailing,
    feats,
    turn,
    d_send,
    d_recv,
    y_send,
    y_recv,
    w_sem,
    tok_sem,
    own_s,
    own_r,
    fwd_s,
    fwd_r,
    kv_s,
    kv_r,
    st_s,
    st_r,
    dd_s,
    dd_r,
    yy_s,
    yy_r,
):
    rows, depth = tok.shape
    width = w_rq.shape[1]
    heads = width // HEAD_DIM
    chips = parts // CORES
    across = row_width(shards)
    me = lax.axis_index("sp")
    t = lax.axis_index("tp")
    chip = t // CORES
    core = t % CORES
    partner = chip * CORES + (1 - core)
    column = me % across
    first = me - column
    chunk = 128 if rows % 128 == 0 else rows
    chunks = rows // chunk
    scale = HEAD_DIM ** (-0.5)

    def tp_at(off):
        return lax.rem(chip + off + chips, chips) * CORES + core

    def at(sp_index, tp_index):
        return {"sp": sp_index, "tp": tp_index}

    order = (w_sk, w_sv, w_sq, w_rk, w_rv, w_rq)
    own_load = pltpu.make_async_copy(tok, xs.at[t], tok_sem)
    own_load.start()
    loads = []
    for i, w in enumerate(order):
        load = pltpu.make_async_copy(w, wall.at[:, pl.ds(i * width, width)], w_sem.at[i])
        load.start()
        loads.append(load)
    out_loads = []
    for i, w in enumerate((o_ret, o_stick)):
        load = pltpu.make_async_copy(w, wo.at[pl.ds(i * width, width), :], w_sem.at[6 + i])
        load.start()
        out_loads.append(load)

    barrier = pltpu.get_barrier_semaphore()

    def greet(sp_index, tp_index):
        pl.semaphore_signal(
            barrier, inc=1, device_id=at(sp_index, tp_index), device_id_type=pl.DeviceIdType.MESH
        )

    greet(me, partner)
    for off in range(1, chips):
        greet(me, tp_at(off))
    for off in range(1, across):
        greet(first + lax.rem(column + off, across), t)
    count = 1 + (chips - 1) + (across - 1)
    for step in (across, 1):
        up = me + step < shards
        down = me - step >= 0

        @pl.when(up)
        def _():
            greet(me + step, t)

        @pl.when(down)
        def _():
            greet(me - step, t)

        count = count + up.astype(jnp.int32) + down.astype(jnp.int32)
    pl.semaphore_wait(barrier, count)

    def remote(src, dst, send, recv, sp_index, tp_index):
        return pltpu.make_async_remote_copy(
            src_ref=src,
            dst_ref=dst,
            send_sem=send,
            recv_sem=recv,
            device_id=at(sp_index, tp_index),
            device_id_type=pl.DeviceIdType.MESH,
        )

    sends = []
    for off in range(1, chips):
        copy = remote(tok, xs.at[t], own_s.at[off], own_r.at[off], me, tp_at(off))
        copy.start()
        sends.append(copy)
    near = remote(tok, xs.at[t], own_s.at[0], own_r.at[0], me, partner)
    near.start()

    lane = lax.broadcasted_iota(jnp.int32, (rows, rows), 1)
    sub = lax.broadcasted_iota(jnp.int32, (rows, rows), 0)
    tri[...] = (sub > lane).astype(BF16)
    for h in range(heads):
        column_ld = jnp.broadcast_to(log_decay[:, h : h + 1], (rows, rows))
        cum_row = jnp.sum(jnp.where(sub <= lane, column_ld, 0.0), axis=0, keepdims=True)
        ld_row = jnp.sum(jnp.where(sub == lane, column_ld, 0.0), axis=0, keepdims=True)
        cum_col = jnp.sum(
            jnp.where(lane <= sub, jnp.broadcast_to(ld_row, (rows, rows)), 0.0),
            axis=1,
            keepdims=True,
        )
        gaps = cum_col - cum_row
        acc[:, pl.ds(h * rows, rows)] = jnp.where(
            lane <= sub, jnp.exp(jnp.where(lane <= sub, gaps, 0.0)), 0.0
        )
        cumb[h] = jnp.broadcast_to(cum_col, (rows, HEAD_DIM))
    for h in range(heads):
        local[h] = acc[:, pl.ds(h * rows, rows)]

    angles = (
        me * rows + lax.broadcasted_iota(jnp.int32, (rows, HEAD_DIM), 0)
    ).astype(F32) * inverse[...]
    left = lax.broadcasted_iota(jnp.int32, (rows, HEAD_DIM), 1) < HEAD_DIM // 2
    sine = jnp.sin(angles)
    turn[0] = jnp.cos(angles)
    turn[1] = jnp.where(left, -sine, sine)

    own_load.wait()
    for load in loads:
        load.wait()

    def weight(j, lo, size):
        return wall[pl.ds(pl.multiple_of(j * depth, depth), depth), pl.ds(lo, size)]

    total = 6 * width
    for i in range(3):
        lo = i * 2 * width
        acc[:, pl.ds(lo, 2 * width)] = dot(xs[t], weight(t, lo, 2 * width))
    near.wait_recv()
    for i in range(3):
        lo = i * 2 * width
        acc[:, pl.ds(lo, 2 * width)] += dot(xs[partner], weight(partner, lo, 2 * width))
    forwards = []
    for off in range(1, chips):
        sends[off - 1].wait_recv()
        j = tp_at(-off)
        copy = remote(xs.at[j], xs.at[j], fwd_s.at[off], fwd_r.at[off], me, partner)
        copy.start()
        forwards.append(copy)
        for i in range(3):
            lo = i * 2 * width
            acc[:, pl.ds(lo, 2 * width)] += dot(xs[j], weight(j, lo, 2 * width))
    far = []
    for off in range(1, chips):
        forwards[off - 1].wait_recv()
        j = tp_at(-off) // CORES * CORES + (1 - core)
        far.append(j)

    def finish(lo, size):
        value = acc[:, pl.ds(lo, size)]
        for j in far:
            value = value + dot(xs[j], weight(j, lo, size))
        return value

    for i in range(2):
        value = finish(i * width, width).astype(BF16)
        for h in range(heads):
            kv[me, h, i] = value[:, h * HEAD_DIM : (h + 1) * HEAD_DIM]

    def block_copy(b, h, slot, target):
        return remote(
            kv.at[b, h], kv.at[b, h], kv_s.at[b, slot, h], kv_r.at[b, h], target, t
        )

    def spread(b, h, act):
        mine = lax.rem(b, across) == column

        @pl.when(jnp.logical_and(mine, me + across < shards))
        def _():
            act(block_copy(b, h, 0, me + across))

        for off in range(1, across):
            target = first + lax.rem(column + off, across)

            @pl.when(jnp.logical_and(mine, jnp.logical_or(b < me, target > me)))
            def _():
                act(block_copy(b, h, off, target))

    for h in range(heads):
        spread(me, h, lambda copy: copy.start())

    sq[...] = finish(2 * width, width).astype(BF16)
    rk = finish(3 * width, width).astype(BF16).astype(F32)
    retv[...] = finish(4 * width, width).astype(BF16)
    rq = finish(5 * width, width).astype(BF16).astype(F32)
    cos, sin = turn[0], turn[1]
    for h in range(heads):
        part = slice(h * HEAD_DIM, (h + 1) * HEAD_DIM)
        q, k = rq[:, part], rk[:, part]
        q = (q * cos + pltpu.roll(q, HEAD_DIM // 2, 1) * sin).astype(BF16)
        k = ((k * cos + pltpu.roll(k, HEAD_DIM // 2, 1) * sin) * scale).astype(BF16)
        qrot[h] = q
        v = retv[:, part]
        scores = (nt(q, k) * local[h]).astype(BF16)
        cum = cumb[h]
        end = cum[rows - 1 : rows, :]
        weighted = (k.astype(F32) * jnp.exp(end - cum)).astype(BF16)
        fresh[h] = dot(weighted.T, v)
        running[h] = dot(scores, v)
    for h in range(heads):
        local[h, :, pl.ds(0, HEAD_DIM)] = running[h]
    running[...] = jnp.zeros_like(running)
    trailing[...] = jnp.zeros_like(trailing)

    def stick(b, diagonal, chunk=rows, chunks=1):
        def one(r, carry):
            at_r = pl.ds(r * chunk, chunk)
            for h in range(heads):
                if not diagonal:

                    @pl.when(lax.rem(b, across) != column)
                    def _():
                        block_copy(b, h, 0, me).wait_recv()

                part = pl.ds(h * HEAD_DIM, HEAD_DIM)
                logits = nt(sq[at_r, part], kv[b, h, 0]) * scale + bias[h]
                soft = jnp.log(1.0 + jnp.exp(-jnp.abs(logits)))
                success = jnp.minimum(logits, 0.0) - soft
                failure = -jnp.maximum(logits, 0.0) - soft
                if diagonal:
                    seen = lax.broadcasted_iota(jnp.int32, (chunk, rows), 1) < (
                        lax.broadcasted_iota(jnp.int32, (chunk, rows), 0) + r * chunk
                    )
                    failure = jnp.where(seen, failure, 0.0)
                high = failure.astype(BF16)
                low = (failure - high.astype(F32)).astype(BF16)
                suffix = dot(high, tri[...]) + dot(low, tri[...])
                weights = jnp.exp(success + suffix)
                if diagonal:
                    weights = jnp.where(seen, weights, 0.0)
                partial = dot(weights.astype(BF16), kv[b, h, 1])
                behind = trailing[h, at_r, :]
                running[h, at_r, :] += jnp.exp(behind) * partial
                trailing[h, at_r, :] = behind + jnp.broadcast_to(
                    suffix[:, 0:1] + failure[:, 0:1], (chunk, HEAD_DIM)
                )
            return carry

        one(0, 0)

    def chain():
        arriving = remote(st_out, st_in, st_s, st_r, me + 1, t)

        @pl.when(me > 0)
        def _():
            arriving.wait_recv()

        @pl.when(me == 0)
        def _():
            st_in[...] = jnp.zeros_like(st_in)

        @pl.when(me + 1 < shards)
        def _():
            for h in range(heads):
                end = cumb[h, pl.ds(rows - 1, 1), :]
                st_out[h] = (jnp.exp(end) * st_in[h].astype(F32) + fresh[h]).astype(BF16)
            arriving.start()

        for h in range(heads):
            carried = dot(qrot[h], st_in[h]) * jnp.exp(cumb[h])
            feats[:, pl.ds(h * HEAD_DIM, HEAD_DIM)] = head_norm(
                local[h, :, pl.ds(0, HEAD_DIM)] + carried
            ).astype(BF16)

    stick(me, True)
    plane = me // across

    def visit(s, carry):
        k, i = s // across, lax.rem(s, across)
        b = (plane - k) * across + (across - 1 - i)

        @pl.when(jnp.logical_and(i == 0, k < plane))
        def _():
            nxt = me - (k + 1) * across
            for h in range(heads):
                block_copy(nxt, h, 0, me).wait_recv()
                spread(nxt, h, lambda copy: copy.start())

        @pl.when(jnp.logical_and(k == plane, i == column))
        def _():
            chain()

        @pl.when(b < me)
        def _():
            stick(b, False)

        return carry

    lax.fori_loop(0, (plane + 1) * across, visit, 0)

    for h in range(heads):
        feats[:, pl.ds(width + h * HEAD_DIM, HEAD_DIM)] = head_norm(running[h]).astype(BF16)

    for load in out_loads:
        load.wait()
    offs = tuple(range(1, chips)) + (0,)

    def project(r, target):
        columns = pl.ds(pl.multiple_of(target * depth, depth), depth)
        return dot(feats[pl.ds(r * chunk, chunk), :], wo[:, columns])

    def pair_copy(off, r):
        cut = pl.ds(r * chunk, chunk)
        return remote(
            d_send.at[off, cut, :], d_recv.at[off, cut, :], dd_s.at[off, r], dd_r.at[off, r], me, partner
        )

    def far_copy(off, r):
        cut = pl.ds(r * chunk, chunk)
        return remote(
            y_send.at[off, cut, :],
            y_recv.at[off, cut, :],
            yy_s.at[off, r],
            yy_r.at[off, r],
            me,
            tp_at(off),
        )

    def send_half(off):
        target = tp_at(off) // CORES * CORES + (1 - core)
        for r in range(chunks):
            d_send[off, pl.ds(r * chunk, chunk), :] = project(r, target).astype(BF16)
            pair_copy(off, r).start()

    send_half(offs[0])
    for n, off in enumerate(offs):
        for r in range(chunks):
            cut = pl.ds(r * chunk, chunk)
            value = project(r, tp_at(off))
            pair_copy(off, r).wait_recv()
            value = value + d_recv[off, cut, :].astype(F32)
            if off:
                y_send[off, cut, :] = value.astype(BF16)
                far_copy(off, r).start()
            else:
                acc[cut, pl.ds(0, depth)] = value
        if n + 1 < len(offs):
            send_half(offs[n + 1])
    for r in range(chunks):
        cut = pl.ds(r * chunk, chunk)
        value = acc[cut, pl.ds(0, depth)]
        for off in range(1, chips):
            far_copy(off, r).wait_recv()
            value = value + y_recv[off, cut, :].astype(F32)
        out[cut, :] = value.astype(BF16)

    near.wait_send()
    for copy in sends + forwards:
        copy.wait_send()

    def drain(s, carry):
        for h in range(heads):
            spread(me - s, h, lambda copy: copy.wait_send())
        return carry

    lax.fori_loop(0, me + 1, drain, 0)

    @pl.when(me + 1 < shards)
    def _():
        remote(st_out, st_in, st_s, st_r, me + 1, t).wait_send()

    for off in offs:
        for r in range(chunks):
            pair_copy(off, r).wait_send()
            if off:
                far_copy(off, r).wait_send()


def body(
    tokens,
    ret_query,
    ret_key,
    ret_value,
    stick_query,
    stick_key,
    stick_value,
    log_decay,
    stick_bias,
    out_ret,
    out_stick,
):
    shards, parts = lax.axis_size("sp"), lax.axis_size("tp")
    rows, depth = tokens.shape
    width = ret_query.shape[1]
    heads = width // HEAD_DIM
    chips = parts // CORES
    across = row_width(shards)
    chunk = 128 if rows % 128 == 0 else rows
    chunks = rows // chunk
    half = HEAD_DIM // 2
    inverse = np.float32(ROPE_BASE) ** (-np.arange(half, dtype=np.float32) / np.float32(half))
    inverse = jnp.asarray(np.tile(inverse, 2)[None, :], F32)
    any_spec = pl.BlockSpec(memory_space=pl.ANY)
    vmem = pl.BlockSpec(memory_space=pltpu.VMEM)
    dma = pltpu.SemaphoreType.DMA
    return pl.pallas_call(
        functools.partial(kernel, shards, parts),
        out_shape=jax.ShapeDtypeStruct((rows, depth), BF16),
        in_specs=[any_spec] * 9 + [vmem] * 2 + [pl.BlockSpec(memory_space=pltpu.SMEM)],
        out_specs=vmem,
        scratch_shapes=[
            pltpu.VMEM((parts, rows, depth), BF16),
            pltpu.VMEM((parts * depth, 6 * width), BF16),
            pltpu.VMEM((2 * width, parts * depth), BF16),
            pltpu.VMEM((rows, max(6 * width, heads * rows, depth)), F32),
            pltpu.VMEM((shards, heads, 2, rows, HEAD_DIM), BF16),
            pltpu.VMEM((rows, width), BF16),
            pltpu.VMEM((heads, rows, HEAD_DIM), BF16),
            pltpu.VMEM((rows, width), BF16),
            pltpu.VMEM((heads, rows, rows), F32),
            pltpu.VMEM((rows, rows), BF16),
            pltpu.VMEM((heads, rows, HEAD_DIM), F32),
            pltpu.VMEM((heads, HEAD_DIM, HEAD_DIM), F32),
            pltpu.VMEM((heads, HEAD_DIM, HEAD_DIM), BF16),
            pltpu.VMEM((heads, HEAD_DIM, HEAD_DIM), BF16),
            pltpu.VMEM((heads, rows, HEAD_DIM), F32),
            pltpu.VMEM((heads, rows, HEAD_DIM), F32),
            pltpu.VMEM((rows, 2 * width), BF16),
            pltpu.VMEM((2, rows, HEAD_DIM), F32),
            pltpu.VMEM((chips, rows, depth), BF16),
            pltpu.VMEM((chips, rows, depth), BF16),
            pltpu.VMEM((chips, rows, depth), BF16),
            pltpu.VMEM((chips, rows, depth), BF16),
            dma((8,)),
            dma,
            dma((chips,)),
            dma((chips,)),
            dma((chips,)),
            dma((chips,)),
            dma((shards, across, heads)),
            dma((shards, heads)),
            dma,
            dma,
            dma((chips, chunks)),
            dma((chips, chunks)),
            dma((chips, chunks)),
            dma((chips, chunks)),
        ],
        compiler_params=pltpu.CompilerParams(
            collective_id=0, has_side_effects=True, vmem_limit_bytes=60000 * 1024
        ),
    )(
        tokens,
        ret_query,
        ret_key,
        ret_value,
        stick_query,
        stick_key,
        stick_value,
        out_ret,
        out_stick,
        log_decay,
        inverse,
        stick_bias,
    )


def wide_kernel(
    shards,
    parts,
    tok,
    w_rq,
    w_rk,
    w_rv,
    w_sq,
    w_sk,
    w_sv,
    o_ret,
    o_stick,
    log_decay,
    inverse,
    bias,
    out,
    xs,
    wall,
    wo,
    kv,
    kv_out,
    q_all,
    q_out,
    q_far,
    far_run,
    far_past,
    far_out,
    far_in,
    ret_q,
    ret_k,
    ret_v,
    decay,
    tri,
    cumb,
    local,
    fresh_out,
    fresh_in,
    end_out,
    end_in,
    plane_out,
    plane_end,
    plane_in,
    ends_in,
    state_at,
    st_side,
    st_own,
    running,
    trailing,
    turn,
    f_ret,
    s_out,
    f_stick,
    acc,
    w_sem,
    wo_sem,
    tok_sem,
    own_s,
    own_r,
    fwd_s,
    fwd_r,
    kx_s,
    kx_r,
    kz_s,
    kz_r,
    q_s,
    q_r,
    qf_s,
    qf_r,
    fb_s,
    fb_r,
    fr_s,
    fr_r,
    en_s,
    en_r,
    sz_s,
    sz_r,
    se_s,
    se_r,
    sx_s,
    sx_r,
    wy_s,
    wx_s,
    ww_r,
    rf_s,
    rf_r,
    rp_s,
    rp_r,
    fd_s,
    fd_r,
    fp_s,
    fp_r,
):
    rows, depth = tok.shape
    width = w_rq.shape[1]
    heads = width // HEAD_DIM
    chips = parts // CORES
    across = row_width(shards)
    planes = shards // across
    me = lax.axis_index("sp")
    t = lax.axis_index("tp")
    chip = t // CORES
    core = t % CORES
    partner = chip * CORES + (1 - core)
    x = me % across
    z = me // across
    first = me - x
    chunk = CHUNK
    chunks = rows // chunk
    bit = BIT
    bits = rows // bit
    plane_rows = across * rows
    tiles = plane_rows // TILE
    scale = HEAD_DIM ** (-0.5)
    last = planes - 1

    def chip_at(off):
        return lax.rem(chip + off, chips)

    def tp_at(off):
        return chip_at(off) * CORES + core

    def col_at(off):
        return lax.rem(x + off, across)

    def cut_of(c):
        return pl.ds(c * chunk, chunk)

    def bit_of(c):
        return pl.ds(c * bit, bit)

    def remote(src, dst, send, recv, sp_index, tp_index):
        return pltpu.make_async_remote_copy(
            src_ref=src,
            dst_ref=dst,
            send_sem=send,
            recv_sem=recv,
            device_id={"sp": sp_index, "tp": tp_index},
            device_id_type=pl.DeviceIdType.MESH,
        )

    own_load = pltpu.make_async_copy(tok, xs.at[t], tok_sem)
    own_load.start()

    barrier = pltpu.get_barrier_semaphore()

    def greet(sp_index, tp_index):
        pl.semaphore_signal(
            barrier,
            inc=1,
            device_id={"sp": sp_index, "tp": tp_index},
            device_id_type=pl.DeviceIdType.MESH,
        )

    for off in range(1, parts):
        greet(me, lax.rem(t + off, parts))
    for off in range(1, shards):
        greet(lax.rem(me + off, shards), t)
    for joff in range(1, across):
        for off in range(1, chips):
            greet(first + col_at(joff), tp_at(off))
    count = (parts - 1) + (shards - 1) + (across - 1) * (chips - 1)
    up = z < last
    down = z > 0
    upper = z >= 2
    lower = z + 2 < planes
    own_load.wait()
    for i, w in enumerate((w_sk, w_sv, w_sq, w_rk, w_rv, w_rq)):
        pltpu.make_async_copy(w, wall.at[:, pl.ds(i * width, width)], w_sem.at[i // 2]).start()

    def weights_in(i):
        at = wall.at[:, pl.ds(2 * i * width, 2 * width)]
        pltpu.make_async_copy(at, at, w_sem.at[i]).wait()

    pl.semaphore_wait(barrier, count)

    def token_copy(off, c):
        at = xs.at[t, bit_of(c), :]
        target = tp_at(off) if off else partner
        return remote(at, at, own_s.at[off], own_r.at[off, c], me, target)

    def token_forward(off, c):
        at = xs.at[tp_at(-off + chips), bit_of(c), :]
        return remote(at, at, fwd_s.at[off], fwd_r.at[off, c], me, partner)

    for c in range(bits):
        for off in tuple(range(1, chips)) + (0,):
            token_copy(off, c).start()

    mixers = (o_ret, o_stick)
    def near_weight(m):
        return remote(
            mixers[m].at[:, pl.ds(pl.multiple_of(partner * depth, depth), depth)],
            wo.at[m, pl.ds(pl.multiple_of(t * width, width), width), :],
            wy_s,
            ww_r.at[2],
            me,
            partner,
        )

    def share_at(s, share):
        lo = s * width + share * HEAD_DIM
        return pl.ds(pl.multiple_of(lo, HEAD_DIM), HEAD_DIM)

    def far_weight(m, off, k):
        j = chip_at(off) * CORES + k
        return remote(
            mixers[m].at[
                pl.ds(pl.multiple_of(x * HEAD_DIM, HEAD_DIM), HEAD_DIM),
                pl.ds(pl.multiple_of(j * depth, depth), depth),
            ],
            wo.at[m, share_at(t, x), :],
            wy_s,
            ww_r.at[m],
            me,
            j,
        )

    def side_weight(m, s, off):
        at = wo.at[m, share_at(s, x), :]
        return remote(at, at, wx_s.at[m], ww_r.at[3 + m], first + col_at(off), t)

    def arrival(at, sem):
        pltpu.make_async_copy(at, at, sem).wait()

    far_tp = [
        chip_at(off) * CORES + k for off in range(1, chips) for k in range(CORES)
    ]

    side_rows = pl.ds(0, len(far_tp) * (across - 1) * HEAD_DIM)

    def relay_weights(m):
        arrival(wo.at[0, pl.ds(0, len(far_tp) * HEAD_DIM), :], ww_r.at[m])
        for s in far_tp:
            for off in range(1, across):
                side_weight(m, s, off).start()

    for m in range(2):
        for off in range(1, chips):
            for k in range(CORES):
                far_weight(m, off, k).start()
        near_weight(m).start()
    own_out = []
    for m in range(2):
        load = pltpu.make_async_copy(
            mixers[m].at[:, pl.ds(pl.multiple_of(t * depth, depth), depth)],
            wo.at[m, pl.ds(pl.multiple_of(t * width, width), width), :],
            wo_sem.at[m],
        )
        load.start()
        own_out.append(load)

    lane = lax.broadcasted_iota(jnp.int32, (rows, rows), 1)
    sub = lax.broadcasted_iota(jnp.int32, (rows, rows), 0)
    for h in range(heads):
        ld_row = jnp.broadcast_to(log_decay[h : h + 1, :], (rows, rows))
        cum_col = jnp.sum(jnp.where(lane <= sub, ld_row, 0.0), axis=1, keepdims=True)
        ld_col = jnp.sum(jnp.where(sub == lane, ld_row, 0.0), axis=1, keepdims=True)
        cum_row = jnp.sum(
            jnp.where(sub <= lane, jnp.broadcast_to(ld_col, (rows, rows)), 0.0),
            axis=0,
            keepdims=True,
        )
        gaps = cum_col - cum_row
        decay[h] = jnp.where(lane <= sub, jnp.exp(jnp.where(lane <= sub, gaps, 0.0)), 0.0)
        cumb[h] = jnp.broadcast_to(cum_col, (rows, HEAD_DIM))
    tri[...] = (
        lax.broadcasted_iota(jnp.int32, (TILE, TILE), 0)
        > lax.broadcasted_iota(jnp.int32, (TILE, TILE), 1)
    ).astype(BF16)

    angles = (
        me * rows + lax.broadcasted_iota(jnp.int32, (rows, HEAD_DIM), 0)
    ).astype(F32) * inverse[...]
    left = lax.broadcasted_iota(jnp.int32, (rows, HEAD_DIM), 1) < HEAD_DIM // 2
    sine = jnp.sin(angles)
    turn[0] = jnp.cos(angles)
    turn[1] = jnp.where(left, -sine, sine)

    def weight(j, lo, size):
        return wall[pl.ds(pl.multiple_of(j * depth, depth), depth), pl.ds(lo, size)]

    def plane_cut(j, c):
        return pl.ds(pl.multiple_of(j * rows + c * chunk, chunk), chunk)

    def plane_bit(j, c):
        return pl.ds(pl.multiple_of(j * rows + c * bit, bit), bit)

    def plane_rows_of(j):
        return pl.ds(pl.multiple_of(j * rows, rows), rows)

    def kx_copy(off, c, col):
        j = col_at(off)
        return remote(
            kv_out.at[j, :, bit_of(c), :],
            kv.at[0, :, plane_bit(col, c), :],
            kx_s.at[off],
            kx_r.at[col, c],
            first + j,
            t,
        )

    def kz_copy(j, c):
        return remote(
            kv.at[0, :, plane_bit(j, c), :],
            kv.at[1, :, plane_bit(j, c), :],
            kz_s,
            kz_r,
            me + across,
            t,
        )

    def relay_x(c):
        for off in range(1, across):
            kx_copy(off, c, col_at(off)).wait_recv()

            @pl.when(up)
            def _():
                kz_copy(col_at(off), c).start()

    def q_copy(off, c, col):
        j = col_at(off)
        return remote(
            q_out.at[j, cut_of(c), :],
            q_all.at[plane_cut(col, c), :],
            q_s.at[off],
            q_r.at[col],
            first + j,
            t,
        )

    def far_q(off, c, col):
        j = col_at(off)
        return remote(
            q_out.at[j, cut_of(c), :],
            q_far.at[plane_cut(col, c), :],
            qf_s,
            qf_r,
            first - 2 * across + j,
            t,
        )

    def far_back(r):
        at = pl.ds(r * TILE, TILE)
        return remote(
            far_out.at[at, :], far_in.at[at, :], fb_s, fb_r.at[r], me + 2 * across, t
        )

    def turned(u, cut):
        return u * turn[0, cut, :] + pltpu.roll(u, HEAD_DIM // 2, 1) * turn[1, cut, :]

    def projected(lo, size, cut):
        value = dot(xs[sources[0], cut, :], weight(sources[0], lo, size))
        for j in sources[1:]:
            value = value + dot(xs[j, cut, :], weight(j, lo, size))
        return value

    def project_q(c):
        cut = cut_of(c)
        value = (projected(2 * width, width, cut) * (scale * LOG2E)).astype(BF16)
        for h in range(heads):
            q_out[h, cut, :] = value[:, h * HEAD_DIM : (h + 1) * HEAD_DIM]

        @pl.when(upper)
        def _():
            for off in range(across - 1, -1, -1):
                far_q(off, c, x).start()

        for off in range(1, across):
            q_copy(off, c, x).start()
        q_all[plane_cut(x, c), :] = q_out[x, cut, :]

    def project_kv(c):
        cut = cut_of(c)
        value = projected(3 * width, 2 * width, cut).astype(BF16)
        for h in range(heads):
            lo = h * HEAD_DIM
            ret_k[h, cut, :] = (
                turned(value[:, lo : lo + HEAD_DIM].astype(F32), cut) * scale
            ).astype(BF16)
            ret_v[h, cut, :] = value[:, width + lo : width + lo + HEAD_DIM]

    def project_rq(c):
        cut = cut_of(c)
        value = projected(5 * width, width, cut).astype(BF16).astype(F32)
        for h in range(heads):
            ret_q[h, cut, :] = turned(value[:, h * HEAD_DIM : (h + 1) * HEAD_DIM], cut).astype(
                BF16
            )

    def relay_down(*items):
        @pl.when(down)
        def _():
            for off, c in items:
                relay_z(z - 1, col_at(off), c)

    weights_in(0)
    far_same = [tp_at(-off + chips) for off in range(1, chips)]
    far_other = [chip_at(-off + chips) * CORES + (1 - core) for off in range(1, chips)]
    sources = [t, partner] + far_same + far_other
    per_chunk = chunk // bit
    for c in range(bits):
        cut = bit_of(c)
        token_copy(0, c).wait_recv()
        value = dot(xs[t, cut, :], weight(t, 0, 2 * width))
        value = value + dot(xs[partner, cut, :], weight(partner, 0, 2 * width))
        for off in range(1, chips):
            token_copy(off, c).wait_recv()
            token_forward(off, c).start()
            j = far_same[off - 1]
            value = value + dot(xs[j, cut, :], weight(j, 0, 2 * width))
        if c >= 3:
            relay_x(c - 3)
        if c == 2:
            weights_in(1)
            weights_in(2)
        group, side = (c - per_chunk) // per_chunk, (c - per_chunk) % per_chunk
        if group >= 0:
            if side == 0:
                project_q(group)
                project_rq(group)
            if side == per_chunk - 1:
                project_kv(group)
        for off in range(1, chips):
            token_forward(off, c).wait_recv()
            j = far_other[off - 1]
            value = value + dot(xs[j, cut, :], weight(j, 0, 2 * width))
        value = value.astype(BF16)
        for i in range(2):
            for h in range(heads):
                lo = i * width + h * HEAD_DIM
                kv_out[h, i, cut, :] = value[:, lo : lo + HEAD_DIM]

        for off in range(1, across):
            kx_copy(off, c, x).start()
        for i in range(2):
            kv[0, i, plane_bit(x, c), :] = kv_out[x, i, cut, :]

        @pl.when(up)
        def _():
            kz_copy(x, c).start()


    project_q(chunks - 1)
    relay_x(bits - 3)
    project_kv(chunks - 1)
    for h in range(heads):
        cum = cumb[h]
        end = cum[rows - 1 : rows, :]
        weighted = (ret_k[h].astype(F32) * jnp.exp(end - cum)).astype(BF16)
        fresh_out[h] = dot(weighted.T, ret_v[h]).astype(BF16)
        end_out[h] = jnp.broadcast_to(jnp.exp(end), (8, HEAD_DIM))

    def fresh_copy(off, col):
        j = col_at(off)
        return remote(
            fresh_out.at[j], fresh_in.at[col], fr_s.at[off], fr_r.at[col], first + j, t
        )

    def end_copy(off, col):
        j = col_at(off)
        return remote(end_out.at[j], end_in.at[col], en_s.at[off], en_r.at[col], first + j, t)

    for off in range(1, across):
        fresh_copy(off, x).start()
        end_copy(off, x).start()

    relay_x(bits - 2)
    project_rq(chunks - 1)
    relay_x(bits - 1)
    for h in range(heads):
        scores = (nt(ret_q[h], ret_k[h]) * decay[h]).astype(BF16)
        local[h] = dot(scores, ret_v[h])
    running[...] = jnp.zeros_like(running)
    trailing[...] = jnp.zeros_like(trailing)
    shift = bias[x] * LOG2E

    def stick(r, p, b, diagonal, query=q_all, total=running, past=trailing):
        at_r = pl.ds(r * TILE, TILE)
        at_b = pl.ds(pl.multiple_of(b * TILE, TILE), TILE)
        logits = nt(query[at_r, :], kv[p, 0, at_b, :]) + shift
        soft = jnp.maximum(
            logits, jnp.log(1.0 + jnp.exp2(jnp.minimum(logits, CLIP))) * LOG2E
        )
        taken = logits - soft
        if diagonal:
            seen = lax.broadcasted_iota(jnp.int32, (TILE, TILE), 1) < lax.broadcasted_iota(
                jnp.int32, (TILE, TILE), 0
            )
            soft = jnp.where(seen, soft, 0.0)
        suffix = dot(soft.astype(BF16), tri[...])
        weights = jnp.exp2(taken - suffix)
        if diagonal:
            weights = jnp.where(seen, weights, 0.0)
        partial = dot(weights.astype(BF16), kv[p, 1, at_b, :])
        behind = past[at_r, :]
        total[at_r, :] += jnp.exp2(-behind) * partial
        past[at_r, :] = behind + jnp.broadcast_to(
            suffix[:, 0:1] + soft[:, 0:1], (TILE, HEAD_DIM)
        )

    def summary(p, target):
        return remote(
            plane_out, plane_in.at[p], sz_s.at[target], sz_r.at[p], target * across + x, t
        )

    def summary_end(p, target):
        return remote(
            plane_end, ends_in.at[p], se_s.at[target], se_r.at[p], target * across + x, t
        )

    for off in range(1, across):
        j = col_at(off)
        arrival(q_all.at[plane_rows_of(j), :], q_r.at[j])
    for r in range(tiles):
        for b in range(r, -1, -1):
            stick(r, 0, b, b == r)
    fresh_in[x] = fresh_out[x]
    end_in[x] = end_out[x]
    for off in range(1, across):
        j = col_at(off)
        fresh_copy(off, j).wait_recv()
        end_copy(off, j).wait_recv()
    value = fresh_in[0].astype(F32)
    scales = end_in[0]
    for j in range(1, across):
        value = end_in[j, 0:1, :] * value + fresh_in[j].astype(F32)
        scales = scales * end_in[j]
    plane_out[...] = value.astype(BF16)
    plane_end[...] = scales
    for target in range(planes - 1, 0, -1):

        @pl.when(target > z)
        def _():
            summary(z, target).start()
            summary_end(z, target).start()

    relay_weights(0)

    @pl.when(down)
    def _():
        arrival(kv.at[1], kz_r)


    @pl.when(lower)
    def _():
        arrival(q_far, qf_r)
        far_run[...] = jnp.zeros_like(far_run)
        far_past[...] = jnp.zeros_like(far_past)
        for r in range(tiles):
            for b in range(tiles - 1, -1, -1):
                stick(r, 0, b, False, q_far, far_run, far_past)

            @pl.when(down)
            def _():
                for b in range(tiles - 1, -1, -1):
                    stick(r, 1, b, False, q_far, far_run, far_past)

            at = pl.ds(r * TILE, TILE)
            far_out[at, :] = far_run[at, :].astype(BF16)
            far_back(r).start()

    def state_side(off, col):
        j = col_at(off)
        return remote(st_side.at[j], st_own.at[col], sx_s.at[off], sx_r.at[col], first + j, t)

    def advance():
        state_at[...] = jnp.zeros_like(state_at)
        for p in range(planes - 1):

            @pl.when(p < z)
            def _():
                summary(p, 0).wait_recv()
                summary_end(p, 0).wait_recv()
                state_at[...] = ends_in[p, 0:1, :] * state_at[...] + plane_in[p].astype(F32)

        state = state_at[...]
        for j in range(across):
            st_side[j] = state.astype(BF16)
            state = end_in[j, 0:1, :] * state + fresh_in[j].astype(F32)
        st_own[x] = st_side[x]
        for off in range(1, across):
            state_side(off, x).start()

    def ret_copy(off):
        at = f_ret.at[t]
        target = tp_at(off) if off else partner
        return remote(at, at, rf_s.at[off], rf_r.at[off], me, target)

    def ret_forward(off):
        at = f_ret.at[tp_at(-off + chips)]
        return remote(at, at, rp_s.at[off], rp_r.at[off], me, partner)

    def visit(p, b):
        for r in range(tiles):
            stick(r, p, b, False)


    @pl.when(down)
    def _():
        for b in range(tiles - 1, -1, -1):
            visit(1, b)

    advance()
    relay_weights(1)

    def finish_ret():
        for off in range(1, across):
            state_side(off, col_at(off)).wait_recv()
        for h in range(heads):
            carried = dot(ret_q[h], st_own[h]) * jnp.exp(cumb[h])
            f_ret[t, :, pl.ds(h * HEAD_DIM, HEAD_DIM)] = head_norm(local[h] + carried).astype(
                BF16
            )
        for off in range(chips):
            ret_copy(off).start()

    finish_ret()

    @pl.when(upper)
    def _():
        for r in range(tiles):
            far_back(r).wait_recv()
            at = pl.ds(r * TILE, TILE)
            running[at, :] += jnp.exp2(-trailing[at, :]) * far_in[at, :].astype(F32)

    def direct_copy(off, joff, c):
        j = col_at(joff)
        return remote(
            s_out.at[j, cut_of(c), :],
            f_stick.at[t, x, cut_of(c), :],
            fd_s.at[off],
            fd_r.at[chip, x, c],
            first + j,
            tp_at(off),
        )

    def direct_arrival(off, joff, c):
        k, j = chip_at(off), col_at(joff)
        return remote(
            s_out.at[j, cut_of(c), :],
            f_stick.at[k * CORES + core, j, cut_of(c), :],
            fd_s.at[off],
            fd_r.at[k, j, c],
            first + j,
            tp_at(off),
        )

    def pair_copy(off, joff, c, side):
        k, j = chip_at(off), col_at(joff)
        at = f_stick.at[k * CORES + side, j, cut_of(c), :]
        return remote(at, at, fp_s, fp_r.at[c], me, partner)

    routes = [(off, joff) for joff in range(across - 1, -1, -1) for off in range(chips - 1, -1, -1)]
    for c in range(chunks):
        for joff in range(across - 1, -1, -1):
            j = col_at(joff)
            value = head_norm(running[plane_cut(j, c), :]).astype(BF16)
            s_out[j, cut_of(c), :] = value
            if joff == 0:
                f_stick[t, x, cut_of(c), :] = value
            for off in range(chips - 1, -1, -1):
                if off or joff:
                    direct_copy(off, joff, c).start()
                else:
                    pair_copy(0, 0, c, core).start()

    for off in range(1, chips):
        ret_copy(off).wait_recv()
        ret_forward(off).start()
    ret_copy(0).wait_recv()
    for load in own_out:
        load.wait()
    arrival(wo.at[0, pl.ds(0, 2 * width), :], ww_r.at[2])
    for m in range(2):
        arrival(wo.at[m, side_rows, :], ww_r.at[3 + m])
    for off in range(1, chips):
        ret_forward(off).wait_recv()
    features = jnp.concatenate([f_ret[s] for s in range(parts)], axis=1)
    acc[...] = dot(features, wo[0])

    for c in range(chunks):
        for off, joff in routes:
            if off or joff:
                direct_arrival(off, joff, c).wait_recv()
                pair_copy(off, joff, c, core).start()
    for c in range(chunks):
        cut = cut_of(c)
        arrival(f_stick.at[pl.ds(0, chips), :, cut, :], fp_r.at[c])
        features = jnp.concatenate(
            [f_stick[s, j, cut, :] for s in range(parts) for j in range(across)], axis=1
        )
        out[cut, :] = (acc[cut, :] + dot(features, wo[1])).astype(BF16)

    for off in range(chips):
        arrival(xs.at[0], own_s.at[off])
        if off:
            arrival(xs.at[0], fwd_s.at[off])
            arrival(f_stick.at[0], fd_s.at[off])
        ret_copy(off).wait_send()
        if off:
            ret_forward(off).wait_send()
    arrival(f_stick.at[0, pl.ds(0, across - 1)], fd_s.at[0])
    arrival(f_stick.at[pl.ds(0, chips)], fp_s)
    arrival(wo.at[0], wy_s)
    for m in range(2):
        arrival(wo.at[m, side_rows, :], wx_s.at[m])
    for off in range(1, across):
        arrival(kv_out.at[0], kx_s.at[off])
        arrival(q_out.at[0], q_s.at[off])
        fresh_copy(off, x).wait_send()
        end_copy(off, x).wait_send()
        state_side(off, x).wait_send()
    for target in range(1, planes):

        @pl.when(target > z)
        def _():
            summary(z, target).wait_send()
            summary_end(z, target).wait_send()

    @pl.when(up)
    def _():
        arrival(kv.at[0], kz_s)

    @pl.when(lower)
    def _():
        arrival(far_out, fb_s)

    @pl.when(upper)
    def _():
        arrival(q_out, qf_s)


def wide_body(
    tokens,
    ret_query,
    ret_key,
    ret_value,
    stick_query,
    stick_key,
    stick_value,
    log_decay,
    stick_bias,
    out_ret,
    out_stick,
):
    shards, parts = lax.axis_size("sp"), lax.axis_size("tp")
    rows, depth = tokens.shape
    width = ret_query.shape[1]
    heads = width // HEAD_DIM
    chips = parts // CORES
    across = row_width(shards)
    planes = shards // across
    chunks = rows // CHUNK
    bits = rows // BIT
    plane_rows = across * rows
    half = HEAD_DIM // 2
    inverse = np.float32(ROPE_BASE) ** (-np.arange(half, dtype=np.float32) / np.float32(half))
    inverse = jnp.asarray(np.tile(inverse, 2)[None, :], F32)
    any_spec = pl.BlockSpec(memory_space=pl.ANY)
    vmem = pl.BlockSpec(memory_space=pltpu.VMEM)
    dma = pltpu.SemaphoreType.DMA
    square = (HEAD_DIM, HEAD_DIM)
    return pl.pallas_call(
        functools.partial(wide_kernel, shards, parts),
        out_shape=jax.ShapeDtypeStruct((rows, depth), BF16),
        in_specs=[any_spec] * 9 + [vmem] * 2 + [pl.BlockSpec(memory_space=pltpu.SMEM)],
        out_specs=vmem,
        scratch_shapes=[
            pltpu.VMEM((parts, rows, depth), BF16),
            pltpu.VMEM((parts * depth, 6 * width), BF16),
            pltpu.VMEM((2, parts * width, depth), BF16),
            pltpu.VMEM((2, 2, plane_rows, HEAD_DIM), BF16),
            pltpu.VMEM((across, 2, rows, HEAD_DIM), BF16),
            pltpu.VMEM((plane_rows, HEAD_DIM), BF16),
            pltpu.VMEM((across, rows, HEAD_DIM), BF16),
            pltpu.VMEM((plane_rows, HEAD_DIM), BF16),
            pltpu.VMEM((plane_rows, HEAD_DIM), F32),
            pltpu.VMEM((plane_rows, HEAD_DIM), F32),
            pltpu.VMEM((plane_rows, HEAD_DIM), BF16),
            pltpu.VMEM((plane_rows, HEAD_DIM), BF16),
            pltpu.VMEM((heads, rows, HEAD_DIM), BF16),
            pltpu.VMEM((heads, rows, HEAD_DIM), BF16),
            pltpu.VMEM((heads, rows, HEAD_DIM), BF16),
            pltpu.VMEM((heads, rows, rows), F32),
            pltpu.VMEM((TILE, TILE), BF16),
            pltpu.VMEM((heads, rows, HEAD_DIM), F32),
            pltpu.VMEM((heads, rows, HEAD_DIM), F32),
            pltpu.VMEM((heads,) + square, BF16),
            pltpu.VMEM((across,) + square, BF16),
            pltpu.VMEM((heads, 8, HEAD_DIM), F32),
            pltpu.VMEM((across, 8, HEAD_DIM), F32),
            pltpu.VMEM(square, BF16),
            pltpu.VMEM((8, HEAD_DIM), F32),
            pltpu.VMEM((planes,) + square, BF16),
            pltpu.VMEM((planes, 8, HEAD_DIM), F32),
            pltpu.VMEM(square, F32),
            pltpu.VMEM((across,) + square, BF16),
            pltpu.VMEM((across,) + square, BF16),
            pltpu.VMEM((plane_rows, HEAD_DIM), F32),
            pltpu.VMEM((plane_rows, HEAD_DIM), F32),
            pltpu.VMEM((2, rows, HEAD_DIM), F32),
            pltpu.VMEM((parts, rows, width), BF16),
            pltpu.VMEM((across, rows, HEAD_DIM), BF16),
            pltpu.VMEM((parts, across, rows, HEAD_DIM), BF16),
            pltpu.VMEM((rows, depth), F32),
            dma((3,)),
            dma((2,)),
            dma,
            dma((chips,)),
            dma((chips, bits)),
            dma((chips,)),
            dma((chips, bits)),
            dma((across,)),
            dma((across, bits)),
            dma,
            dma,
            dma((across,)),
            dma((across,)),
            dma,
            dma,
            dma,
            dma((plane_rows // TILE,)),
            dma((across,)),
            dma((across,)),
            dma((across,)),
            dma((across,)),
            dma((planes,)),
            dma((planes,)),
            dma((planes,)),
            dma((planes,)),
            dma((across,)),
            dma((across,)),
            dma,
            dma((2,)),
            dma((5,)),
            dma((chips,)),
            dma((chips,)),
            dma((chips,)),
            dma((chips,)),
            dma((chips,)),
            dma((chips, across, chunks)),
            dma,
            dma((chunks,)),
        ],
        compiler_params=pltpu.CompilerParams(
            collective_id=0, has_side_effects=True, vmem_limit_bytes=60000 * 1024
        ),
    )(
        tokens,
        ret_query,
        ret_key,
        ret_value,
        stick_query,
        stick_key,
        stick_value,
        out_ret,
        out_stick,
        log_decay.T,
        inverse,
        stick_bias,
    )


def pick(tokens, ret_query, *rest):
    shards = lax.axis_size("sp")
    rows, heads = tokens.shape[0], ret_query.shape[1] // HEAD_DIM
    across = row_width(shards)
    wide = heads == across and rows % CHUNK == 0 and (across * rows) % TILE == 0 and shards == 4 * across
    return (wide_body if wide else body)(tokens, ret_query, *rest)


def solution(mesh):
    in_specs = (
        P("sp", "tp"),
        P(None, "tp"),
        P(None, "tp"),
        P(None, "tp"),
        P(None, "tp"),
        P(None, "tp"),
        P(None, "tp"),
        P("sp", "tp"),
        P("tp"),
        P("tp", None),
        P("tp", None),
    )
    return jax.shard_map(
        pick, mesh=mesh, in_specs=in_specs, out_specs=P("sp", "tp"), check_vma=False
    )
```

```python
import functools

import jax
import jax.numpy as jnp
import numpy as np
from jax import lax
from jax.experimental import pallas as pl
from jax.experimental.pallas import tpu as pltpu
from jax.sharding import PartitionSpec as P

HEAD_DIM = 128
EPS = 1e-05
ROPE_BASE = 10000.0
CORES = 2
CHUNK = 128
BIT = 64
TILE = 256
LOG2E = 1.4426950408889634
CLIP = 40.0
F32 = jnp.float32
BF16 = jnp.bfloat16


def row_width(shards):
    width = 1
    while (2 * width) ** 2 <= shards and shards % (2 * width) == 0:
        width *= 2
    return width


def head_norm(values):
    centred = values - jnp.mean(values, axis=-1, keepdims=True)
    spread = jnp.mean(centred * centred, axis=-1, keepdims=True)
    return centred * lax.rsqrt(spread + EPS)


def nt(a, b):
    return lax.dot_general(a, b, (((1,), (1,)), ((), ())), preferred_element_type=F32)


def dot(a, b):
    return jnp.dot(a, b, preferred_element_type=F32)


def kernel(
    shards,
    parts,
    tok,
    w_rq,
    w_rk,
    w_rv,
    w_sq,
    w_sk,
    w_sv,
    o_ret,
    o_stick,
    log_decay,
    inverse,
    bias,
    out,
    xs,
    wall,
    wo,
    acc,
    kv,
    sq,
    qrot,
    retv,
    local,
    tri,
    cumb,
    fresh,
    st_in,
    st_out,
    running,
    trailing,
    feats,
    turn,
    d_send,
    d_recv,
    y_send,
    y_recv,
    w_sem,
    tok_sem,
    own_s,
    own_r,
    fwd_s,
    fwd_r,
    kv_s,
    kv_r,
    st_s,
    st_r,
    dd_s,
    dd_r,
    yy_s,
    yy_r,
):
    rows, depth = tok.shape
    width = w_rq.shape[1]
    heads = width // HEAD_DIM
    chips = parts // CORES
    across = row_width(shards)
    me = lax.axis_index("sp")
    t = lax.axis_index("tp")
    chip = t // CORES
    core = t % CORES
    partner = chip * CORES + (1 - core)
    column = me % across
    first = me - column
    chunk = 128 if rows % 128 == 0 else rows
    chunks = rows // chunk
    scale = HEAD_DIM ** (-0.5)

    def tp_at(off):
        return lax.rem(chip + off + chips, chips) * CORES + core

    def at(sp_index, tp_index):
        return {"sp": sp_index, "tp": tp_index}

    order = (w_sk, w_sv, w_sq, w_rk, w_rv, w_rq)
    own_load = pltpu.make_async_copy(tok, xs.at[t], tok_sem)
    own_load.start()
    loads = []
    for i, w in enumerate(order):
        load = pltpu.make_async_copy(w, wall.at[:, pl.ds(i * width, width)], w_sem.at[i])
        load.start()
        loads.append(load)
    out_loads = []
    for i, w in enumerate((o_ret, o_stick)):
        load = pltpu.make_async_copy(w, wo.at[pl.ds(i * width, width), :], w_sem.at[6 + i])
        load.start()
        out_loads.append(load)

    barrier = pltpu.get_barrier_semaphore()

    def greet(sp_index, tp_index):
        pl.semaphore_signal(
            barrier, inc=1, device_id=at(sp_index, tp_index), device_id_type=pl.DeviceIdType.MESH
        )

    greet(me, partner)
    for off in range(1, chips):
        greet(me, tp_at(off))
    for off in range(1, across):
        greet(first + lax.rem(column + off, across), t)
    count = 1 + (chips - 1) + (across - 1)
    for step in (across, 1):
        up = me + step < shards
        down = me - step >= 0

        @pl.when(up)
        def _():
            greet(me + step, t)

        @pl.when(down)
        def _():
            greet(me - step, t)

        count = count + up.astype(jnp.int32) + down.astype(jnp.int32)
    pl.semaphore_wait(barrier, count)

    def remote(src, dst, send, recv, sp_index, tp_index):
        return pltpu.make_async_remote_copy(
            src_ref=src,
            dst_ref=dst,
            send_sem=send,
            recv_sem=recv,
            device_id=at(sp_index, tp_index),
            device_id_type=pl.DeviceIdType.MESH,
        )

    sends = []
    for off in range(1, chips):
        copy = remote(tok, xs.at[t], own_s.at[off], own_r.at[off], me, tp_at(off))
        copy.start()
        sends.append(copy)
    near = remote(tok, xs.at[t], own_s.at[0], own_r.at[0], me, partner)
    near.start()

    lane = lax.broadcasted_iota(jnp.int32, (rows, rows), 1)
    sub = lax.broadcasted_iota(jnp.int32, (rows, rows), 0)
    tri[...] = (sub > lane).astype(BF16)
    for h in range(heads):
        column_ld = jnp.broadcast_to(log_decay[:, h : h + 1], (rows, rows))
        cum_row = jnp.sum(jnp.where(sub <= lane, column_ld, 0.0), axis=0, keepdims=True)
        ld_row = jnp.sum(jnp.where(sub == lane, column_ld, 0.0), axis=0, keepdims=True)
        cum_col = jnp.sum(
            jnp.where(lane <= sub, jnp.broadcast_to(ld_row, (rows, rows)), 0.0),
            axis=1,
            keepdims=True,
        )
        gaps = cum_col - cum_row
        acc[:, pl.ds(h * rows, rows)] = jnp.where(
            lane <= sub, jnp.exp(jnp.where(lane <= sub, gaps, 0.0)), 0.0
        )
        cumb[h] = jnp.broadcast_to(cum_col, (rows, HEAD_DIM))
    for h in range(heads):
        local[h] = acc[:, pl.ds(h * rows, rows)]

    angles = (
        me * rows + lax.broadcasted_iota(jnp.int32, (rows, HEAD_DIM), 0)
    ).astype(F32) * inverse[...]
    left = lax.broadcasted_iota(jnp.int32, (rows, HEAD_DIM), 1) < HEAD_DIM // 2
    sine = jnp.sin(angles)
    turn[0] = jnp.cos(angles)
    turn[1] = jnp.where(left, -sine, sine)

    own_load.wait()
    for load in loads:
        load.wait()

    def weight(j, lo, size):
        return wall[pl.ds(pl.multiple_of(j * depth, depth), depth), pl.ds(lo, size)]

    total = 6 * width
    for i in range(3):
        lo = i * 2 * width
        acc[:, pl.ds(lo, 2 * width)] = dot(xs[t], weight(t, lo, 2 * width))
    near.wait_recv()
    for i in range(3):
        lo = i * 2 * width
        acc[:, pl.ds(lo, 2 * width)] += dot(xs[partner], weight(partner, lo, 2 * width))
    forwards = []
    for off in range(1, chips):
        sends[off - 1].wait_recv()
        j = tp_at(-off)
        copy = remote(xs.at[j], xs.at[j], fwd_s.at[off], fwd_r.at[off], me, partner)
        copy.start()
        forwards.append(copy)
        for i in range(3):
            lo = i * 2 * width
            acc[:, pl.ds(lo, 2 * width)] += dot(xs[j], weight(j, lo, 2 * width))
    far = []
    for off in range(1, chips):
        forwards[off - 1].wait_recv()
        j = tp_at(-off) // CORES * CORES + (1 - core)
        far.append(j)

    def finish(lo, size):
        value = acc[:, pl.ds(lo, size)]
        for j in far:
            value = value + dot(xs[j], weight(j, lo, size))
        return value

    for i in range(2):
        value = finish(i * width, width).astype(BF16)
        for h in range(heads):
            kv[me, h, i] = value[:, h * HEAD_DIM : (h + 1) * HEAD_DIM]

    def block_copy(b, h, slot, target):
        return remote(
            kv.at[b, h], kv.at[b, h], kv_s.at[b, slot, h], kv_r.at[b, h], target, t
        )

    def spread(b, h, act):
        mine = lax.rem(b, across) == column

        @pl.when(jnp.logical_and(mine, me + across < shards))
        def _():
            act(block_copy(b, h, 0, me + across))

        for off in range(1, across):
            target = first + lax.rem(column + off, across)

            @pl.when(jnp.logical_and(mine, jnp.logical_or(b < me, target > me)))
            def _():
                act(block_copy(b, h, off, target))

    for h in range(heads):
        spread(me, h, lambda copy: copy.start())

    sq[...] = finish(2 * width, width).astype(BF16)
    rk = finish(3 * width, width).astype(BF16).astype(F32)
    retv[...] = finish(4 * width, width).astype(BF16)
    rq = finish(5 * width, width).astype(BF16).astype(F32)
    cos, sin = turn[0], turn[1]
    for h in range(heads):
        part = slice(h * HEAD_DIM, (h + 1) * HEAD_DIM)
        q, k = rq[:, part], rk[:, part]
        q = (q * cos + pltpu.roll(q, HEAD_DIM // 2, 1) * sin).astype(BF16)
        k = ((k * cos + pltpu.roll(k, HEAD_DIM // 2, 1) * sin) * scale).astype(BF16)
        qrot[h] = q
        v = retv[:, part]
        scores = (nt(q, k) * local[h]).astype(BF16)
        cum = cumb[h]
        end = cum[rows - 1 : rows, :]
        weighted = (k.astype(F32) * jnp.exp(end - cum)).astype(BF16)
        fresh[h] = dot(weighted.T, v)
        running[h] = dot(scores, v)
    for h in range(heads):
        local[h, :, pl.ds(0, HEAD_DIM)] = running[h]
    running[...] = jnp.zeros_like(running)
    trailing[...] = jnp.zeros_like(trailing)

    def stick(b, diagonal, chunk=rows, chunks=1):
        def one(r, carry):
            at_r = pl.ds(r * chunk, chunk)
            for h in range(heads):
                if not diagonal:

                    @pl.when(lax.rem(b, across) != column)
                    def _():
                        block_copy(b, h, 0, me).wait_recv()

                part = pl.ds(h * HEAD_DIM, HEAD_DIM)
                logits = nt(sq[at_r, part], kv[b, h, 0]) * scale + bias[h]
                soft = jnp.log(1.0 + jnp.exp(-jnp.abs(logits)))
                success = jnp.minimum(logits, 0.0) - soft
                failure = -jnp.maximum(logits, 0.0) - soft
                if diagonal:
                    seen = lax.broadcasted_iota(jnp.int32, (chunk, rows), 1) < (
                        lax.broadcasted_iota(jnp.int32, (chunk, rows), 0) + r * chunk
                    )
                    failure = jnp.where(seen, failure, 0.0)
                high = failure.astype(BF16)
                low = (failure - high.astype(F32)).astype(BF16)
                suffix = dot(high, tri[...]) + dot(low, tri[...])
                weights = jnp.exp(success + suffix)
                if diagonal:
                    weights = jnp.where(seen, weights, 0.0)
                partial = dot(weights.astype(BF16), kv[b, h, 1])
                behind = trailing[h, at_r, :]
                running[h, at_r, :] += jnp.exp(behind) * partial
                trailing[h, at_r, :] = behind + jnp.broadcast_to(
                    suffix[:, 0:1] + failure[:, 0:1], (chunk, HEAD_DIM)
                )
            return carry

        one(0, 0)

    def chain():
        arriving = remote(st_out, st_in, st_s, st_r, me + 1, t)

        @pl.when(me > 0)
        def _():
            arriving.wait_recv()

        @pl.when(me == 0)
        def _():
            st_in[...] = jnp.zeros_like(st_in)

        @pl.when(me + 1 < shards)
        def _():
            for h in range(heads):
                end = cumb[h, pl.ds(rows - 1, 1), :]
                st_out[h] = (jnp.exp(end) * st_in[h].astype(F32) + fresh[h]).astype(BF16)
            arriving.start()

        for h in range(heads):
            carried = dot(qrot[h], st_in[h]) * jnp.exp(cumb[h])
            feats[:, pl.ds(h * HEAD_DIM, HEAD_DIM)] = head_norm(
                local[h, :, pl.ds(0, HEAD_DIM)] + carried
            ).astype(BF16)

    stick(me, True)
    plane = me // across

    def visit(s, carry):
        k, i = s // across, lax.rem(s, across)
        b = (plane - k) * across + (across - 1 - i)

        @pl.when(jnp.logical_and(i == 0, k < plane))
        def _():
            nxt = me - (k + 1) * across
            for h in range(heads):
                block_copy(nxt, h, 0, me).wait_recv()
                spread(nxt, h, lambda copy: copy.start())

        @pl.when(jnp.logical_and(k == plane, i == column))
        def _():
            chain()

        @pl.when(b < me)
        def _():
            stick(b, False)

        return carry

    lax.fori_loop(0, (plane + 1) * across, visit, 0)

    for h in range(heads):
        feats[:, pl.ds(width + h * HEAD_DIM, HEAD_DIM)] = head_norm(running[h]).astype(BF16)

    for load in out_loads:
        load.wait()
    offs = tuple(range(1, chips)) + (0,)

    def project(r, target):
        columns = pl.ds(pl.multiple_of(target * depth, depth), depth)
        return dot(feats[pl.ds(r * chunk, chunk), :], wo[:, columns])

    def pair_copy(off, r):
        cut = pl.ds(r * chunk, chunk)
        return remote(
            d_send.at[off, cut, :], d_recv.at[off, cut, :], dd_s.at[off, r], dd_r.at[off, r], me, partner
        )

    def far_copy(off, r):
        cut = pl.ds(r * chunk, chunk)
        return remote(
            y_send.at[off, cut, :],
            y_recv.at[off, cut, :],
            yy_s.at[off, r],
            yy_r.at[off, r],
            me,
            tp_at(off),
        )

    def send_half(off):
        target = tp_at(off) // CORES * CORES + (1 - core)
        for r in range(chunks):
            d_send[off, pl.ds(r * chunk, chunk), :] = project(r, target).astype(BF16)
            pair_copy(off, r).start()

    send_half(offs[0])
    for n, off in enumerate(offs):
        for r in range(chunks):
            cut = pl.ds(r * chunk, chunk)
            value = project(r, tp_at(off))
            pair_copy(off, r).wait_recv()
            value = value + d_recv[off, cut, :].astype(F32)
            if off:
                y_send[off, cut, :] = value.astype(BF16)
                far_copy(off, r).start()
            else:
                acc[cut, pl.ds(0, depth)] = value
        if n + 1 < len(offs):
            send_half(offs[n + 1])
    for r in range(chunks):
        cut = pl.ds(r * chunk, chunk)
        value = acc[cut, pl.ds(0, depth)]
        for off in range(1, chips):
            far_copy(off, r).wait_recv()
            value = value + y_recv[off, cut, :].astype(F32)
        out[cut, :] = value.astype(BF16)

    near.wait_send()
    for copy in sends + forwards:
        copy.wait_send()

    def drain(s, carry):
        for h in range(heads):
            spread(me - s, h, lambda copy: copy.wait_send())
        return carry

    lax.fori_loop(0, me + 1, drain, 0)

    @pl.when(me + 1 < shards)
    def _():
        remote(st_out, st_in, st_s, st_r, me + 1, t).wait_send()

    for off in offs:
        for r in range(chunks):
            pair_copy(off, r).wait_send()
            if off:
                far_copy(off, r).wait_send()


def body(
    tokens,
    ret_query,
    ret_key,
    ret_value,
    stick_query,
    stick_key,
    stick_value,
    log_decay,
    stick_bias,
    out_ret,
    out_stick,
):
    shards, parts = lax.axis_size("sp"), lax.axis_size("tp")
    rows, depth = tokens.shape
    width = ret_query.shape[1]
    heads = width // HEAD_DIM
    chips = parts // CORES
    across = row_width(shards)
    chunk = 128 if rows % 128 == 0 else rows
    chunks = rows // chunk
    half = HEAD_DIM // 2
    inverse = np.float32(ROPE_BASE) ** (-np.arange(half, dtype=np.float32) / np.float32(half))
    inverse = jnp.asarray(np.tile(inverse, 2)[None, :], F32)
    any_spec = pl.BlockSpec(memory_space=pl.ANY)
    vmem = pl.BlockSpec(memory_space=pltpu.VMEM)
    dma = pltpu.SemaphoreType.DMA
    return pl.pallas_call(
        functools.partial(kernel, shards, parts),
        out_shape=jax.ShapeDtypeStruct((rows, depth), BF16),
        in_specs=[any_spec] * 9 + [vmem] * 2 + [pl.BlockSpec(memory_space=pltpu.SMEM)],
        out_specs=vmem,
        scratch_shapes=[
            pltpu.VMEM((parts, rows, depth), BF16),
            pltpu.VMEM((parts * depth, 6 * width), BF16),
            pltpu.VMEM((2 * width, parts * depth), BF16),
            pltpu.VMEM((rows, max(6 * width, heads * rows, depth)), F32),
            pltpu.VMEM((shards, heads, 2, rows, HEAD_DIM), BF16),
            pltpu.VMEM((rows, width), BF16),
            pltpu.VMEM((heads, rows, HEAD_DIM), BF16),
            pltpu.VMEM((rows, width), BF16),
            pltpu.VMEM((heads, rows, rows), F32),
            pltpu.VMEM((rows, rows), BF16),
            pltpu.VMEM((heads, rows, HEAD_DIM), F32),
            pltpu.VMEM((heads, HEAD_DIM, HEAD_DIM), F32),
            pltpu.VMEM((heads, HEAD_DIM, HEAD_DIM), BF16),
            pltpu.VMEM((heads, HEAD_DIM, HEAD_DIM), BF16),
            pltpu.VMEM((heads, rows, HEAD_DIM), F32),
            pltpu.VMEM((heads, rows, HEAD_DIM), F32),
            pltpu.VMEM((rows, 2 * width), BF16),
            pltpu.VMEM((2, rows, HEAD_DIM), F32),
            pltpu.VMEM((chips, rows, depth), BF16),
            pltpu.VMEM((chips, rows, depth), BF16),
            pltpu.VMEM((chips, rows, depth), BF16),
            pltpu.VMEM((chips, rows, depth), BF16),
            dma((8,)),
            dma,
            dma((chips,)),
            dma((chips,)),
            dma((chips,)),
            dma((chips,)),
            dma((shards, across, heads)),
            dma((shards, heads)),
            dma,
            dma,
            dma((chips, chunks)),
            dma((chips, chunks)),
            dma((chips, chunks)),
            dma((chips, chunks)),
        ],
        compiler_params=pltpu.CompilerParams(
            collective_id=0, has_side_effects=True, vmem_limit_bytes=60000 * 1024
        ),
    )(
        tokens,
        ret_query,
        ret_key,
        ret_value,
        stick_query,
        stick_key,
        stick_value,
        out_ret,
        out_stick,
        log_decay,
        inverse,
        stick_bias,
    )


def wide_kernel(
    shards,
    parts,
    tok,
    w_rq,
    w_rk,
    w_rv,
    w_sq,
    w_sk,
    w_sv,
    o_ret,
    o_stick,
    log_decay,
    inverse,
    bias,
    out,
    xs,
    wall,
    wo,
    kv,
    kv_out,
    q_all,
    q_out,
    q_far,
    far_run,
    far_past,
    far_out,
    far_in,
    ret_q,
    ret_k,
    ret_v,
    decay,
    tri,
    cumb,
    local,
    fresh_out,
    fresh_in,
    end_out,
    end_in,
    plane_out,
    plane_end,
    plane_in,
    ends_in,
    state_at,
    st_side,
    st_own,
    running,
    trailing,
    turn,
    f_ret,
    s_out,
    f_stick,
    acc,
    w_sem,
    wo_sem,
    tok_sem,
    own_s,
    own_r,
    fwd_s,
    fwd_r,
    kx_s,
    kx_r,
    kz_s,
    kz_r,
    q_s,
    q_r,
    qf_s,
    qf_r,
    fb_s,
    fb_r,
    fr_s,
    fr_r,
    en_s,
    en_r,
    sz_s,
    sz_r,
    se_s,
    se_r,
    sx_s,
    sx_r,
    wy_s,
    wx_s,
    ww_r,
    rf_s,
    rf_r,
    rp_s,
    rp_r,
    fd_s,
    fd_r,
    fp_s,
    fp_r,
):
    rows, depth = tok.shape
    width = w_rq.shape[1]
    heads = width // HEAD_DIM
    chips = parts // CORES
    across = row_width(shards)
    planes = shards // across
    me = lax.axis_index("sp")
    t = lax.axis_index("tp")
    chip = t // CORES
    core = t % CORES
    partner = chip * CORES + (1 - core)
    x = me % across
    z = me // across
    first = me - x
    chunk = CHUNK
    chunks = rows // chunk
    bit = BIT
    bits = rows // bit
    plane_rows = across * rows
    tiles = plane_rows // TILE
    scale = HEAD_DIM ** (-0.5)
    last = planes - 1

    def chip_at(off):
        return lax.rem(chip + off, chips)

    def tp_at(off):
        return chip_at(off) * CORES + core

    def col_at(off):
        return lax.rem(x + off, across)

    def cut_of(c):
        return pl.ds(c * chunk, chunk)

    def bit_of(c):
        return pl.ds(c * bit, bit)

    def remote(src, dst, send, recv, sp_index, tp_index):
        return pltpu.make_async_remote_copy(
            src_ref=src,
            dst_ref=dst,
            send_sem=send,
            recv_sem=recv,
            device_id={"sp": sp_index, "tp": tp_index},
            device_id_type=pl.DeviceIdType.MESH,
        )

    own_load = pltpu.make_async_copy(tok, xs.at[t], tok_sem)
    own_load.start()

    barrier = pltpu.get_barrier_semaphore()

    def greet(sp_index, tp_index):
        pl.semaphore_signal(
            barrier,
            inc=1,
            device_id={"sp": sp_index, "tp": tp_index},
            device_id_type=pl.DeviceIdType.MESH,
        )

    for off in range(1, parts):
        greet(me, lax.rem(t + off, parts))
    for off in range(1, shards):
        greet(lax.rem(me + off, shards), t)
    for joff in range(1, across):
        for off in range(1, chips):
            greet(first + col_at(joff), tp_at(off))
    count = (parts - 1) + (shards - 1) + (across - 1) * (chips - 1)
    up = z < last
    down = z > 0
    upper = z >= 2
    lower = z + 2 < planes
    own_load.wait()
    for i, w in enumerate((w_sk, w_sv, w_sq, w_rk, w_rv, w_rq)):
        pltpu.make_async_copy(w, wall.at[:, pl.ds(i * width, width)], w_sem.at[i // 2]).start()

    def weights_in(i):
        at = wall.at[:, pl.ds(2 * i * width, 2 * width)]
        pltpu.make_async_copy(at, at, w_sem.at[i]).wait()

    pl.semaphore_wait(barrier, count)

    def token_copy(off, c):
        at = xs.at[t, bit_of(c), :]
        target = tp_at(off) if off else partner
        return remote(at, at, own_s.at[off], own_r.at[off, c], me, target)

    def token_forward(off, c):
        at = xs.at[tp_at(-off + chips), bit_of(c), :]
        return remote(at, at, fwd_s.at[off], fwd_r.at[off, c], me, partner)

    for c in range(bits):
        for off in tuple(range(1, chips)) + (0,):
            token_copy(off, c).start()

    mixers = (o_ret, o_stick)
    def near_weight(m):
        return remote(
            mixers[m].at[:, pl.ds(pl.multiple_of(partner * depth, depth), depth)],
            wo.at[m, pl.ds(pl.multiple_of(t * width, width), width), :],
            wy_s,
            ww_r.at[2],
            me,
            partner,
        )

    blocks = (width // 2, width // across)
    mine = (z % 2, x)

    def share_at(m, s):
        lo = s * width + mine[m] * blocks[m]
        return pl.ds(pl.multiple_of(lo, HEAD_DIM), blocks[m])

    def far_weight(m, off, k):
        j = chip_at(off) * CORES + k
        return remote(
            mixers[m].at[
                pl.ds(pl.multiple_of(mine[m] * blocks[m], HEAD_DIM), blocks[m]),
                pl.ds(pl.multiple_of(j * depth, depth), depth),
            ],
            wo.at[m, share_at(m, t), :],
            wy_s,
            ww_r.at[m],
            me,
            j,
        )

    def side_weight(m, s, off):
        at = wo.at[m, share_at(m, s), :]
        target = first + col_at(off) if m else me + across * (1 - 2 * mine[0])
        return remote(at, at, wx_s.at[m], ww_r.at[3 + m], target, t)

    def arrival(at, sem):
        pltpu.make_async_copy(at, at, sem).wait()

    far_tp = [
        chip_at(off) * CORES + k for off in range(1, chips) for k in range(CORES)
    ]

    sides = (1, across - 1)

    def side_rows(m):
        return pl.ds(0, len(far_tp) * sides[m] * blocks[m])

    def relay_weights(m):
        arrival(wo.at[0, pl.ds(0, len(far_tp) * blocks[m]), :], ww_r.at[m])
        for s in far_tp:
            for off in range(1, sides[m] + 1):
                side_weight(m, s, off).start()

    for m in range(2):
        for off in range(1, chips):
            for k in range(CORES):
                far_weight(m, off, k).start()
        near_weight(m).start()
    own_out = []
    for m in range(2):
        load = pltpu.make_async_copy(
            mixers[m].at[:, pl.ds(pl.multiple_of(t * depth, depth), depth)],
            wo.at[m, pl.ds(pl.multiple_of(t * width, width), width), :],
            wo_sem.at[m],
        )
        load.start()
        own_out.append(load)

    lane = lax.broadcasted_iota(jnp.int32, (rows, rows), 1)
    sub = lax.broadcasted_iota(jnp.int32, (rows, rows), 0)
    for h in range(heads):
        ld_row = jnp.broadcast_to(log_decay[h : h + 1, :], (rows, rows))
        cum_col = jnp.sum(jnp.where(lane <= sub, ld_row, 0.0), axis=1, keepdims=True)
        ld_col = jnp.sum(jnp.where(sub == lane, ld_row, 0.0), axis=1, keepdims=True)
        cum_row = jnp.sum(
            jnp.where(sub <= lane, jnp.broadcast_to(ld_col, (rows, rows)), 0.0),
            axis=0,
            keepdims=True,
        )
        gaps = cum_col - cum_row
        decay[h] = jnp.where(lane <= sub, jnp.exp(jnp.where(lane <= sub, gaps, 0.0)), 0.0)
        cumb[h] = jnp.broadcast_to(cum_col, (rows, HEAD_DIM))
    tri[...] = (
        lax.broadcasted_iota(jnp.int32, (TILE, TILE), 0)
        > lax.broadcasted_iota(jnp.int32, (TILE, TILE), 1)
    ).astype(BF16)

    angles = (
        me * rows + lax.broadcasted_iota(jnp.int32, (rows, HEAD_DIM), 0)
    ).astype(F32) * inverse[...]
    left = lax.broadcasted_iota(jnp.int32, (rows, HEAD_DIM), 1) < HEAD_DIM // 2
    sine = jnp.sin(angles)
    turn[0] = jnp.cos(angles)
    turn[1] = jnp.where(left, -sine, sine)

    def weight(j, lo, size):
        return wall[pl.ds(pl.multiple_of(j * depth, depth), depth), pl.ds(lo, size)]

    def plane_cut(j, c):
        return pl.ds(pl.multiple_of(j * rows + c * chunk, chunk), chunk)

    def plane_bit(j, c):
        return pl.ds(pl.multiple_of(j * rows + c * bit, bit), bit)

    def plane_rows_of(j):
        return pl.ds(pl.multiple_of(j * rows, rows), rows)

    def kx_copy(off, c, col):
        j = col_at(off)
        return remote(
            kv_out.at[j, :, bit_of(c), :],
            kv.at[0, :, plane_bit(col, c), :],
            kx_s.at[off],
            kx_r.at[col, c],
            first + j,
            t,
        )

    def kz_copy(j, c):
        return remote(
            kv.at[0, :, plane_bit(j, c), :],
            kv.at[1, :, plane_bit(j, c), :],
            kz_s,
            kz_r,
            me + across,
            t,
        )

    def relay_x(c):
        for off in range(1, across):
            kx_copy(off, c, col_at(off)).wait_recv()

            @pl.when(up)
            def _():
                kz_copy(col_at(off), c).start()

    def q_copy(off, c, col):
        j = col_at(off)
        return remote(
            q_out.at[j, cut_of(c), :],
            q_all.at[plane_cut(col, c), :],
            q_s.at[off],
            q_r.at[col],
            first + j,
            t,
        )

    def far_q(off, c, col):
        j = col_at(off)
        return remote(
            q_out.at[j, cut_of(c), :],
            q_far.at[plane_cut(col, c), :],
            qf_s,
            qf_r,
            first - 2 * across + j,
            t,
        )

    def far_back(r):
        at = pl.ds(r * TILE, TILE)
        return remote(
            far_out.at[at, :], far_in.at[at, :], fb_s, fb_r.at[r], me + 2 * across, t
        )

    def turned(u, cut):
        return u * turn[0, cut, :] + pltpu.roll(u, HEAD_DIM // 2, 1) * turn[1, cut, :]

    def projected(lo, size, cut):
        value = dot(xs[sources[0], cut, :], weight(sources[0], lo, size))
        for j in sources[1:]:
            value = value + dot(xs[j, cut, :], weight(j, lo, size))
        return value

    def project_q(c):
        cut = cut_of(c)
        value = (projected(2 * width, width, cut) * (scale * LOG2E)).astype(BF16)
        for h in range(heads):
            q_out[h, cut, :] = value[:, h * HEAD_DIM : (h + 1) * HEAD_DIM]

        @pl.when(upper)
        def _():
            for off in range(across - 1, -1, -1):
                far_q(off, c, x).start()

        for off in range(1, across):
            q_copy(off, c, x).start()
        q_all[plane_cut(x, c), :] = q_out[x, cut, :]

    def project_kv(c):
        cut = cut_of(c)
        value = projected(3 * width, 2 * width, cut).astype(BF16)
        for h in range(heads):
            lo = h * HEAD_DIM
            ret_k[h, cut, :] = (
                turned(value[:, lo : lo + HEAD_DIM].astype(F32), cut) * scale
            ).astype(BF16)
            ret_v[h, cut, :] = value[:, width + lo : width + lo + HEAD_DIM]

    def project_rq(c):
        cut = cut_of(c)
        value = projected(5 * width, width, cut).astype(BF16).astype(F32)
        for h in range(heads):
            ret_q[h, cut, :] = turned(value[:, h * HEAD_DIM : (h + 1) * HEAD_DIM], cut).astype(
                BF16
            )

    def relay_down(*items):
        @pl.when(down)
        def _():
            for off, c in items:
                relay_z(z - 1, col_at(off), c)

    weights_in(0)
    far_same = [tp_at(-off + chips) for off in range(1, chips)]
    far_other = [chip_at(-off + chips) * CORES + (1 - core) for off in range(1, chips)]
    sources = [t, partner] + far_same + far_other
    per_chunk = chunk // bit
    for c in range(bits):
        cut = bit_of(c)
        token_copy(0, c).wait_recv()
        value = dot(xs[t, cut, :], weight(t, 0, 2 * width))
        value = value + dot(xs[partner, cut, :], weight(partner, 0, 2 * width))
        for off in range(1, chips):
            token_copy(off, c).wait_recv()
            token_forward(off, c).start()
            j = far_same[off - 1]
            value = value + dot(xs[j, cut, :], weight(j, 0, 2 * width))
        if c >= 3:
            relay_x(c - 3)
        if c == 2:
            weights_in(1)
            weights_in(2)
        group, side = (c - per_chunk) // per_chunk, (c - per_chunk) % per_chunk
        if group >= 0:
            if side == 0:
                project_q(group)
                project_rq(group)
            if side == per_chunk - 1:
                project_kv(group)
        for off in range(1, chips):
            token_forward(off, c).wait_recv()
            j = far_other[off - 1]
            value = value + dot(xs[j, cut, :], weight(j, 0, 2 * width))
        value = value.astype(BF16)
        for i in range(2):
            for h in range(heads):
                lo = i * width + h * HEAD_DIM
                kv_out[h, i, cut, :] = value[:, lo : lo + HEAD_DIM]

        for off in range(1, across):
            kx_copy(off, c, x).start()
        for i in range(2):
            kv[0, i, plane_bit(x, c), :] = kv_out[x, i, cut, :]

        @pl.when(up)
        def _():
            kz_copy(x, c).start()


    project_q(chunks - 1)
    relay_x(bits - 3)
    project_kv(chunks - 1)
    for h in range(heads):
        cum = cumb[h]
        end = cum[rows - 1 : rows, :]
        weighted = (ret_k[h].astype(F32) * jnp.exp(end - cum)).astype(BF16)
        fresh_out[h] = dot(weighted.T, ret_v[h]).astype(BF16)
        end_out[h] = jnp.broadcast_to(jnp.exp(end), (8, HEAD_DIM))

    def fresh_copy(off, col):
        j = col_at(off)
        return remote(
            fresh_out.at[j], fresh_in.at[col], fr_s.at[off], fr_r.at[col], first + j, t
        )

    def end_copy(off, col):
        j = col_at(off)
        return remote(end_out.at[j], end_in.at[col], en_s.at[off], en_r.at[col], first + j, t)

    for off in range(1, across):
        fresh_copy(off, x).start()
        end_copy(off, x).start()

    relay_x(bits - 2)
    project_rq(chunks - 1)
    relay_x(bits - 1)
    for h in range(heads):
        scores = (nt(ret_q[h], ret_k[h]) * decay[h]).astype(BF16)
        local[h] = dot(scores, ret_v[h])
    running[...] = jnp.zeros_like(running)
    trailing[...] = jnp.zeros_like(trailing)
    shift = bias[x] * LOG2E

    def stick(r, p, b, diagonal, query=q_all, total=running, past=trailing):
        at_r = pl.ds(r * TILE, TILE)
        at_b = pl.ds(pl.multiple_of(b * TILE, TILE), TILE)
        logits = nt(query[at_r, :], kv[p, 0, at_b, :]) + shift
        soft = jnp.maximum(
            logits, jnp.log(1.0 + jnp.exp2(jnp.minimum(logits, CLIP))) * LOG2E
        )
        taken = logits - soft
        if diagonal:
            seen = lax.broadcasted_iota(jnp.int32, (TILE, TILE), 1) < lax.broadcasted_iota(
                jnp.int32, (TILE, TILE), 0
            )
            soft = jnp.where(seen, soft, 0.0)
        suffix = dot(soft.astype(BF16), tri[...])
        weights = jnp.exp2(taken - suffix)
        if diagonal:
            weights = jnp.where(seen, weights, 0.0)
        partial = dot(weights.astype(BF16), kv[p, 1, at_b, :])
        behind = past[at_r, :]
        total[at_r, :] += jnp.exp2(-behind) * partial
        past[at_r, :] = behind + jnp.broadcast_to(
            suffix[:, 0:1] + soft[:, 0:1], (TILE, HEAD_DIM)
        )

    def summary(p, target):
        return remote(
            plane_out, plane_in.at[p], sz_s.at[target], sz_r.at[p], target * across + x, t
        )

    def summary_end(p, target):
        return remote(
            plane_end, ends_in.at[p], se_s.at[target], se_r.at[p], target * across + x, t
        )

    for off in range(1, across):
        j = col_at(off)
        arrival(q_all.at[plane_rows_of(j), :], q_r.at[j])
    for r in range(tiles):
        for b in range(r, -1, -1):
            stick(r, 0, b, b == r)
    fresh_in[x] = fresh_out[x]
    end_in[x] = end_out[x]
    for off in range(1, across):
        j = col_at(off)
        fresh_copy(off, j).wait_recv()
        end_copy(off, j).wait_recv()
    value = fresh_in[0].astype(F32)
    scales = end_in[0]
    for j in range(1, across):
        value = end_in[j, 0:1, :] * value + fresh_in[j].astype(F32)
        scales = scales * end_in[j]
    plane_out[...] = value.astype(BF16)
    plane_end[...] = scales
    for target in range(planes - 1, 0, -1):

        @pl.when(target > z)
        def _():
            summary(z, target).start()
            summary_end(z, target).start()

    def state_side(off, col):
        j = col_at(off)
        return remote(st_side.at[j], st_own.at[col], sx_s.at[off], sx_r.at[col], first + j, t)

    def advance():
        state_at[...] = jnp.zeros_like(state_at)
        for p in range(planes - 1):

            @pl.when(p < z)
            def _():
                summary(p, 0).wait_recv()
                summary_end(p, 0).wait_recv()
                state_at[...] = ends_in[p, 0:1, :] * state_at[...] + plane_in[p].astype(F32)

        state = state_at[...]
        for j in range(across):
            st_side[j] = state.astype(BF16)
            state = end_in[j, 0:1, :] * state + fresh_in[j].astype(F32)
        st_own[x] = st_side[x]
        for off in range(1, across):
            state_side(off, x).start()


    @pl.when(z == 0)
    def _():
        advance()

    relay_weights(0)

    @pl.when(down)
    def _():
        arrival(kv.at[1], kz_r)

    def ret_copy(off):
        at = f_ret.at[t]
        target = tp_at(off) if off else partner
        return remote(at, at, rf_s.at[off], rf_r.at[off], me, target)

    def finish_ret():
        for off in range(1, across):
            state_side(off, col_at(off)).wait_recv()
        for h in range(heads):
            carried = dot(ret_q[h], st_own[h]) * jnp.exp(cumb[h])
            f_ret[t, :, pl.ds(h * HEAD_DIM, HEAD_DIM)] = head_norm(local[h] + carried).astype(
                BF16
            )
        for off in range(chips):
            ret_copy(off).start()


    @pl.when(z == 0)
    def _():
        relay_weights(1)


    @pl.when(lower)
    def _():
        arrival(q_far, qf_r)
        far_run[...] = jnp.zeros_like(far_run)
        far_past[...] = jnp.zeros_like(far_past)
        for r in range(tiles):
            for b in range(tiles - 1, -1, -1):
                stick(r, 0, b, False, q_far, far_run, far_past)

            @pl.when(down)
            def _():
                for b in range(tiles - 1, -1, -1):
                    stick(r, 1, b, False, q_far, far_run, far_past)

            at = pl.ds(r * TILE, TILE)
            far_out[at, :] = far_run[at, :].astype(BF16)
            far_back(r).start()
            if r == max(tiles - 2, 0):

                @pl.when(down)
                def _():
                    advance()

        @pl.when(down)
        def _():
            relay_weights(1)

        finish_ret()

    def ret_forward(off):
        at = f_ret.at[tp_at(-off + chips)]
        return remote(at, at, rp_s.at[off], rp_r.at[off], me, partner)

    def visit(p, b):
        for r in range(tiles):
            stick(r, p, b, False)


    @pl.when(down)
    def _():
        for b in range(tiles - 1, -1, -1):
            visit(1, b)


    @pl.when(upper)
    def _():
        advance()
        relay_weights(1)
        finish_ret()


    def direct_copy(off, j, c):
        return remote(
            s_out.at[j, cut_of(c), :],
            f_stick.at[t, x, cut_of(c), :],
            fd_s.at[off],
            fd_r.at[chip, x, c],
            first + j,
            tp_at(off),
        )

    def pair_copy(off, j, c):
        at = f_stick.at[chip_at(off) * CORES + core, j, cut_of(c), :]
        return remote(at, at, fp_s, fp_r.at[c], me, partner)

    for n in range(across * chunks):
        j, c = n // chunks, n % chunks
        if (n * chunk) % TILE == 0:
            r = n * chunk // TILE

            @pl.when(upper)
            def _():
                far_back(r).wait_recv()
                at = pl.ds(r * TILE, TILE)
                running[at, :] += jnp.exp2(-trailing[at, :]) * far_in[at, :].astype(F32)

        value = head_norm(running[pl.ds(n * chunk, chunk), :]).astype(BF16)
        s_out[j, cut_of(c), :] = value
        for off in range(chips - 1, 0, -1):
            direct_copy(off, j, c).start()

        @pl.when(j == x)
        def _():
            f_stick[t, x, cut_of(c), :] = s_out[j, cut_of(c), :]
            pair_copy(0, x, c).start()

        @pl.when(j != x)
        def _():
            direct_copy(0, j, c).start()

    for off in range(1, chips):
        ret_copy(off).wait_recv()
        ret_forward(off).start()

    def direct_in(c):
        for joff in range(across - 1, -1, -1):
            for off in range(chips):
                if off or joff:
                    k, j = chip_at(off), col_at(joff)
                    arrival(f_stick.at[k * CORES + core, j, cut_of(c), :], fd_r.at[k, j, c])
                    pair_copy(off, j, c).start()

    for c in range(chunks - 1):
        direct_in(c)
    ret_copy(0).wait_recv()
    for load in own_out:
        load.wait()
    arrival(wo.at[0, pl.ds(0, 2 * width), :], ww_r.at[2])
    arrival(wo.at[0, side_rows(0), :], ww_r.at[3])
    for off in range(1, chips):
        ret_forward(off).wait_recv()
    features = jnp.concatenate([f_ret[s] for s in range(parts)], axis=1)
    acc[...] = dot(features, wo[0])
    direct_in(chunks - 1)
    arrival(wo.at[1, side_rows(1), :], ww_r.at[4])
    for c in range(chunks):
        cut = cut_of(c)
        arrival(f_stick.at[pl.ds(0, chips), :, cut, :], fp_r.at[c])
        features = jnp.concatenate(
            [f_stick[s, j, cut, :] for s in range(parts) for j in range(across)], axis=1
        )
        out[cut, :] = (acc[cut, :] + dot(features, wo[1])).astype(BF16)
    for off in range(chips):
        arrival(xs.at[0], own_s.at[off])
        if off:
            arrival(xs.at[0], fwd_s.at[off])
            arrival(f_stick.at[0], fd_s.at[off])
        ret_copy(off).wait_send()
        if off:
            ret_forward(off).wait_send()
    arrival(f_stick.at[0, pl.ds(0, across - 1)], fd_s.at[0])
    arrival(f_stick.at[pl.ds(0, chips)], fp_s)
    sent = 2 * width + len(far_tp) * (blocks[0] + blocks[1])
    arrival(wo.at[0, pl.ds(0, sent), :], wy_s)
    for m in range(2):
        arrival(wo.at[m, side_rows(m), :], wx_s.at[m])
    for off in range(1, across):
        arrival(kv_out.at[0], kx_s.at[off])
        arrival(q_out.at[0], q_s.at[off])
        fresh_copy(off, x).wait_send()
        end_copy(off, x).wait_send()
        state_side(off, x).wait_send()
    for target in range(1, planes):

        @pl.when(target > z)
        def _():
            summary(z, target).wait_send()
            summary_end(z, target).wait_send()

    @pl.when(up)
    def _():
        arrival(kv.at[0], kz_s)

    @pl.when(lower)
    def _():
        arrival(far_out, fb_s)

    @pl.when(upper)
    def _():
        arrival(q_out, qf_s)


def wide_body(
    tokens,
    ret_query,
    ret_key,
    ret_value,
    stick_query,
    stick_key,
    stick_value,
    log_decay,
    stick_bias,
    out_ret,
    out_stick,
):
    shards, parts = lax.axis_size("sp"), lax.axis_size("tp")
    rows, depth = tokens.shape
    width = ret_query.shape[1]
    heads = width // HEAD_DIM
    chips = parts // CORES
    across = row_width(shards)
    planes = shards // across
    chunks = rows // CHUNK
    bits = rows // BIT
    plane_rows = across * rows
    half = HEAD_DIM // 2
    inverse = np.float32(ROPE_BASE) ** (-np.arange(half, dtype=np.float32) / np.float32(half))
    inverse = jnp.asarray(np.tile(inverse, 2)[None, :], F32)
    any_spec = pl.BlockSpec(memory_space=pl.ANY)
    vmem = pl.BlockSpec(memory_space=pltpu.VMEM)
    dma = pltpu.SemaphoreType.DMA
    square = (HEAD_DIM, HEAD_DIM)
    return pl.pallas_call(
        functools.partial(wide_kernel, shards, parts),
        out_shape=jax.ShapeDtypeStruct((rows, depth), BF16),
        in_specs=[any_spec] * 9 + [vmem] * 2 + [pl.BlockSpec(memory_space=pltpu.SMEM)],
        out_specs=vmem,
        scratch_shapes=[
            pltpu.VMEM((parts, rows, depth), BF16),
            pltpu.VMEM((parts * depth, 6 * width), BF16),
            pltpu.VMEM((2, parts * width, depth), BF16),
            pltpu.VMEM((2, 2, plane_rows, HEAD_DIM), BF16),
            pltpu.VMEM((across, 2, rows, HEAD_DIM), BF16),
            pltpu.VMEM((plane_rows, HEAD_DIM), BF16),
            pltpu.VMEM((across, rows, HEAD_DIM), BF16),
            pltpu.VMEM((plane_rows, HEAD_DIM), BF16),
            pltpu.VMEM((plane_rows, HEAD_DIM), F32),
            pltpu.VMEM((plane_rows, HEAD_DIM), F32),
            pltpu.VMEM((plane_rows, HEAD_DIM), BF16),
            pltpu.VMEM((plane_rows, HEAD_DIM), BF16),
            pltpu.VMEM((heads, rows, HEAD_DIM), BF16),
            pltpu.VMEM((heads, rows, HEAD_DIM), BF16),
            pltpu.VMEM((heads, rows, HEAD_DIM), BF16),
            pltpu.VMEM((heads, rows, rows), F32),
            pltpu.VMEM((TILE, TILE), BF16),
            pltpu.VMEM((heads, rows, HEAD_DIM), F32),
            pltpu.VMEM((heads, rows, HEAD_DIM), F32),
            pltpu.VMEM((heads,) + square, BF16),
            pltpu.VMEM((across,) + square, BF16),
            pltpu.VMEM((heads, 8, HEAD_DIM), F32),
            pltpu.VMEM((across, 8, HEAD_DIM), F32),
            pltpu.VMEM(square, BF16),
            pltpu.VMEM((8, HEAD_DIM), F32),
            pltpu.VMEM((planes,) + square, BF16),
            pltpu.VMEM((planes, 8, HEAD_DIM), F32),
            pltpu.VMEM(square, F32),
            pltpu.VMEM((across,) + square, BF16),
            pltpu.VMEM((across,) + square, BF16),
            pltpu.VMEM((plane_rows, HEAD_DIM), F32),
            pltpu.VMEM((plane_rows, HEAD_DIM), F32),
            pltpu.VMEM((2, rows, HEAD_DIM), F32),
            pltpu.VMEM((parts, rows, width), BF16),
            pltpu.VMEM((across, rows, HEAD_DIM), BF16),
            pltpu.VMEM((parts, across, rows, HEAD_DIM), BF16),
            pltpu.VMEM((rows, depth), F32),
            dma((3,)),
            dma((2,)),
            dma,
            dma((chips,)),
            dma((chips, bits)),
            dma((chips,)),
            dma((chips, bits)),
            dma((across,)),
            dma((across, bits)),
            dma,
            dma,
            dma((across,)),
            dma((across,)),
            dma,
            dma,
            dma,
            dma((plane_rows // TILE,)),
            dma((across,)),
            dma((across,)),
            dma((across,)),
            dma((across,)),
            dma((planes,)),
            dma((planes,)),
            dma((planes,)),
            dma((planes,)),
            dma((across,)),
            dma((across,)),
            dma,
            dma((2,)),
            dma((5,)),
            dma((chips,)),
            dma((chips,)),
            dma((chips,)),
            dma((chips,)),
            dma((chips,)),
            dma((chips, across, chunks)),
            dma,
            dma((chunks,)),
        ],
        compiler_params=pltpu.CompilerParams(
            collective_id=0, has_side_effects=True, vmem_limit_bytes=60000 * 1024
        ),
    )(
        tokens,
        ret_query,
        ret_key,
        ret_value,
        stick_query,
        stick_key,
        stick_value,
        out_ret,
        out_stick,
        log_decay.T,
        inverse,
        stick_bias,
    )


def pick(tokens, ret_query, *rest):
    shards = lax.axis_size("sp")
    rows, heads = tokens.shape[0], ret_query.shape[1] // HEAD_DIM
    across = row_width(shards)
    wide = heads == across and rows % CHUNK == 0 and (across * rows) % TILE == 0 and shards == 4 * across
    return (wide_body if wide else body)(tokens, ret_query, *rest)


def solution(mesh):
    in_specs = (
        P("sp", "tp"),
        P(None, "tp"),
        P(None, "tp"),
        P(None, "tp"),
        P(None, "tp"),
        P(None, "tp"),
        P(None, "tp"),
        P("sp", "tp"),
        P("tp"),
        P("tp", None),
        P("tp", None),
    )
    return jax.shard_map(
        pick, mesh=mesh, in_specs=in_specs, out_specs=P("sp", "tp"), check_vma=False
    )
```

```python
import functools

import jax
import jax.numpy as jnp
import numpy as np
from jax import lax
from jax.experimental import pallas as pl
from jax.experimental.pallas import tpu as pltpu
from jax.sharding import PartitionSpec as P

HEAD_DIM = 128
EPS = 1e-05
ROPE_BASE = 10000.0
CORES = 2
CHUNK = 128
BIT = 64
TILE = 256
LOG2E = 1.4426950408889634
CLIP = 40.0
F32 = jnp.float32
BF16 = jnp.bfloat16


def row_width(shards):
    width = 1
    while (2 * width) ** 2 <= shards and shards % (2 * width) == 0:
        width *= 2
    return width


def head_norm(values):
    centred = values - jnp.mean(values, axis=-1, keepdims=True)
    spread = jnp.mean(centred * centred, axis=-1, keepdims=True)
    return centred * lax.rsqrt(spread + EPS)


def nt(a, b):
    return lax.dot_general(a, b, (((1,), (1,)), ((), ())), preferred_element_type=F32)


def dot(a, b):
    return jnp.dot(a, b, preferred_element_type=F32)


def kernel(
    shards,
    parts,
    tok,
    w_rq,
    w_rk,
    w_rv,
    w_sq,
    w_sk,
    w_sv,
    o_ret,
    o_stick,
    log_decay,
    inverse,
    bias,
    out,
    xs,
    wall,
    wo,
    acc,
    kv,
    sq,
    qrot,
    retv,
    local,
    tri,
    cumb,
    fresh,
    st_in,
    st_out,
    running,
    trailing,
    feats,
    turn,
    d_send,
    d_recv,
    y_send,
    y_recv,
    w_sem,
    tok_sem,
    own_s,
    own_r,
    fwd_s,
    fwd_r,
    kv_s,
    kv_r,
    st_s,
    st_r,
    dd_s,
    dd_r,
    yy_s,
    yy_r,
):
    rows, depth = tok.shape
    width = w_rq.shape[1]
    heads = width // HEAD_DIM
    chips = parts // CORES
    across = row_width(shards)
    me = lax.axis_index("sp")
    t = lax.axis_index("tp")
    chip = t // CORES
    core = t % CORES
    partner = chip * CORES + (1 - core)
    column = me % across
    first = me - column
    chunk = 128 if rows % 128 == 0 else rows
    chunks = rows // chunk
    scale = HEAD_DIM ** (-0.5)

    def tp_at(off):
        return lax.rem(chip + off + chips, chips) * CORES + core

    def at(sp_index, tp_index):
        return {"sp": sp_index, "tp": tp_index}

    order = (w_sk, w_sv, w_sq, w_rk, w_rv, w_rq)
    own_load = pltpu.make_async_copy(tok, xs.at[t], tok_sem)
    own_load.start()
    loads = []
    for i, w in enumerate(order):
        load = pltpu.make_async_copy(w, wall.at[:, pl.ds(i * width, width)], w_sem.at[i])
        load.start()
        loads.append(load)
    out_loads = []
    for i, w in enumerate((o_ret, o_stick)):
        load = pltpu.make_async_copy(w, wo.at[pl.ds(i * width, width), :], w_sem.at[6 + i])
        load.start()
        out_loads.append(load)

    barrier = pltpu.get_barrier_semaphore()

    def greet(sp_index, tp_index):
        pl.semaphore_signal(
            barrier, inc=1, device_id=at(sp_index, tp_index), device_id_type=pl.DeviceIdType.MESH
        )

    greet(me, partner)
    for off in range(1, chips):
        greet(me, tp_at(off))
    for off in range(1, across):
        greet(first + lax.rem(column + off, across), t)
    count = 1 + (chips - 1) + (across - 1)
    for step in (across, 1):
        up = me + step < shards
        down = me - step >= 0

        @pl.when(up)
        def _():
            greet(me + step, t)

        @pl.when(down)
        def _():
            greet(me - step, t)

        count = count + up.astype(jnp.int32) + down.astype(jnp.int32)
    pl.semaphore_wait(barrier, count)

    def remote(src, dst, send, recv, sp_index, tp_index):
        return pltpu.make_async_remote_copy(
            src_ref=src,
            dst_ref=dst,
            send_sem=send,
            recv_sem=recv,
            device_id=at(sp_index, tp_index),
            device_id_type=pl.DeviceIdType.MESH,
        )

    sends = []
    for off in range(1, chips):
        copy = remote(tok, xs.at[t], own_s.at[off], own_r.at[off], me, tp_at(off))
        copy.start()
        sends.append(copy)
    near = remote(tok, xs.at[t], own_s.at[0], own_r.at[0], me, partner)
    near.start()

    lane = lax.broadcasted_iota(jnp.int32, (rows, rows), 1)
    sub = lax.broadcasted_iota(jnp.int32, (rows, rows), 0)
    tri[...] = (sub > lane).astype(BF16)
    for h in range(heads):
        column_ld = jnp.broadcast_to(log_decay[:, h : h + 1], (rows, rows))
        cum_row = jnp.sum(jnp.where(sub <= lane, column_ld, 0.0), axis=0, keepdims=True)
        ld_row = jnp.sum(jnp.where(sub == lane, column_ld, 0.0), axis=0, keepdims=True)
        cum_col = jnp.sum(
            jnp.where(lane <= sub, jnp.broadcast_to(ld_row, (rows, rows)), 0.0),
            axis=1,
            keepdims=True,
        )
        gaps = cum_col - cum_row
        acc[:, pl.ds(h * rows, rows)] = jnp.where(
            lane <= sub, jnp.exp(jnp.where(lane <= sub, gaps, 0.0)), 0.0
        )
        cumb[h] = jnp.broadcast_to(cum_col, (rows, HEAD_DIM))
    for h in range(heads):
        local[h] = acc[:, pl.ds(h * rows, rows)]

    angles = (
        me * rows + lax.broadcasted_iota(jnp.int32, (rows, HEAD_DIM), 0)
    ).astype(F32) * inverse[...]
    left = lax.broadcasted_iota(jnp.int32, (rows, HEAD_DIM), 1) < HEAD_DIM // 2
    sine = jnp.sin(angles)
    turn[0] = jnp.cos(angles)
    turn[1] = jnp.where(left, -sine, sine)

    own_load.wait()
    for load in loads:
        load.wait()

    def weight(j, lo, size):
        return wall[pl.ds(pl.multiple_of(j * depth, depth), depth), pl.ds(lo, size)]

    total = 6 * width
    for i in range(3):
        lo = i * 2 * width
        acc[:, pl.ds(lo, 2 * width)] = dot(xs[t], weight(t, lo, 2 * width))
    near.wait_recv()
    for i in range(3):
        lo = i * 2 * width
        acc[:, pl.ds(lo, 2 * width)] += dot(xs[partner], weight(partner, lo, 2 * width))
    forwards = []
    for off in range(1, chips):
        sends[off - 1].wait_recv()
        j = tp_at(-off)
        copy = remote(xs.at[j], xs.at[j], fwd_s.at[off], fwd_r.at[off], me, partner)
        copy.start()
        forwards.append(copy)
        for i in range(3):
            lo = i * 2 * width
            acc[:, pl.ds(lo, 2 * width)] += dot(xs[j], weight(j, lo, 2 * width))
    far = []
    for off in range(1, chips):
        forwards[off - 1].wait_recv()
        j = tp_at(-off) // CORES * CORES + (1 - core)
        far.append(j)

    def finish(lo, size):
        value = acc[:, pl.ds(lo, size)]
        for j in far:
            value = value + dot(xs[j], weight(j, lo, size))
        return value

    for i in range(2):
        value = finish(i * width, width).astype(BF16)
        for h in range(heads):
            kv[me, h, i] = value[:, h * HEAD_DIM : (h + 1) * HEAD_DIM]

    def block_copy(b, h, slot, target):
        return remote(
            kv.at[b, h], kv.at[b, h], kv_s.at[b, slot, h], kv_r.at[b, h], target, t
        )

    def spread(b, h, act):
        mine = lax.rem(b, across) == column

        @pl.when(jnp.logical_and(mine, me + across < shards))
        def _():
            act(block_copy(b, h, 0, me + across))

        for off in range(1, across):
            target = first + lax.rem(column + off, across)

            @pl.when(jnp.logical_and(mine, jnp.logical_or(b < me, target > me)))
            def _():
                act(block_copy(b, h, off, target))

    for h in range(heads):
        spread(me, h, lambda copy: copy.start())

    sq[...] = finish(2 * width, width).astype(BF16)
    rk = finish(3 * width, width).astype(BF16).astype(F32)
    retv[...] = finish(4 * width, width).astype(BF16)
    rq = finish(5 * width, width).astype(BF16).astype(F32)
    cos, sin = turn[0], turn[1]
    for h in range(heads):
        part = slice(h * HEAD_DIM, (h + 1) * HEAD_DIM)
        q, k = rq[:, part], rk[:, part]
        q = (q * cos + pltpu.roll(q, HEAD_DIM // 2, 1) * sin).astype(BF16)
        k = ((k * cos + pltpu.roll(k, HEAD_DIM // 2, 1) * sin) * scale).astype(BF16)
        qrot[h] = q
        v = retv[:, part]
        scores = (nt(q, k) * local[h]).astype(BF16)
        cum = cumb[h]
        end = cum[rows - 1 : rows, :]
        weighted = (k.astype(F32) * jnp.exp(end - cum)).astype(BF16)
        fresh[h] = dot(weighted.T, v)
        running[h] = dot(scores, v)
    for h in range(heads):
        local[h, :, pl.ds(0, HEAD_DIM)] = running[h]
    running[...] = jnp.zeros_like(running)
    trailing[...] = jnp.zeros_like(trailing)

    def stick(b, diagonal, chunk=rows, chunks=1):
        def one(r, carry):
            at_r = pl.ds(r * chunk, chunk)
            for h in range(heads):
                if not diagonal:

                    @pl.when(lax.rem(b, across) != column)
                    def _():
                        block_copy(b, h, 0, me).wait_recv()

                part = pl.ds(h * HEAD_DIM, HEAD_DIM)
                logits = nt(sq[at_r, part], kv[b, h, 0]) * scale + bias[h]
                soft = jnp.log(1.0 + jnp.exp(-jnp.abs(logits)))
                success = jnp.minimum(logits, 0.0) - soft
                failure = -jnp.maximum(logits, 0.0) - soft
                if diagonal:
                    seen = lax.broadcasted_iota(jnp.int32, (chunk, rows), 1) < (
                        lax.broadcasted_iota(jnp.int32, (chunk, rows), 0) + r * chunk
                    )
                    failure = jnp.where(seen, failure, 0.0)
                high = failure.astype(BF16)
                low = (failure - high.astype(F32)).astype(BF16)
                suffix = dot(high, tri[...]) + dot(low, tri[...])
                weights = jnp.exp(success + suffix)
                if diagonal:
                    weights = jnp.where(seen, weights, 0.0)
                partial = dot(weights.astype(BF16), kv[b, h, 1])
                behind = trailing[h, at_r, :]
                running[h, at_r, :] += jnp.exp(behind) * partial
                trailing[h, at_r, :] = behind + jnp.broadcast_to(
                    suffix[:, 0:1] + failure[:, 0:1], (chunk, HEAD_DIM)
                )
            return carry

        one(0, 0)

    def chain():
        arriving = remote(st_out, st_in, st_s, st_r, me + 1, t)

        @pl.when(me > 0)
        def _():
            arriving.wait_recv()

        @pl.when(me == 0)
        def _():
            st_in[...] = jnp.zeros_like(st_in)

        @pl.when(me + 1 < shards)
        def _():
            for h in range(heads):
                end = cumb[h, pl.ds(rows - 1, 1), :]
                st_out[h] = (jnp.exp(end) * st_in[h].astype(F32) + fresh[h]).astype(BF16)
            arriving.start()

        for h in range(heads):
            carried = dot(qrot[h], st_in[h]) * jnp.exp(cumb[h])
            feats[:, pl.ds(h * HEAD_DIM, HEAD_DIM)] = head_norm(
                local[h, :, pl.ds(0, HEAD_DIM)] + carried
            ).astype(BF16)

    stick(me, True)
    plane = me // across

    def visit(s, carry):
        k, i = s // across, lax.rem(s, across)
        b = (plane - k) * across + (across - 1 - i)

        @pl.when(jnp.logical_and(i == 0, k < plane))
        def _():
            nxt = me - (k + 1) * across
            for h in range(heads):
                block_copy(nxt, h, 0, me).wait_recv()
                spread(nxt, h, lambda copy: copy.start())

        @pl.when(jnp.logical_and(k == plane, i == column))
        def _():
            chain()

        @pl.when(b < me)
        def _():
            stick(b, False)

        return carry

    lax.fori_loop(0, (plane + 1) * across, visit, 0)

    for h in range(heads):
        feats[:, pl.ds(width + h * HEAD_DIM, HEAD_DIM)] = head_norm(running[h]).astype(BF16)

    for load in out_loads:
        load.wait()
    offs = tuple(range(1, chips)) + (0,)

    def project(r, target):
        columns = pl.ds(pl.multiple_of(target * depth, depth), depth)
        return dot(feats[pl.ds(r * chunk, chunk), :], wo[:, columns])

    def pair_copy(off, r):
        cut = pl.ds(r * chunk, chunk)
        return remote(
            d_send.at[off, cut, :], d_recv.at[off, cut, :], dd_s.at[off, r], dd_r.at[off, r], me, partner
        )

    def far_copy(off, r):
        cut = pl.ds(r * chunk, chunk)
        return remote(
            y_send.at[off, cut, :],
            y_recv.at[off, cut, :],
            yy_s.at[off, r],
            yy_r.at[off, r],
            me,
            tp_at(off),
        )

    def send_half(off):
        target = tp_at(off) // CORES * CORES + (1 - core)
        for r in range(chunks):
            d_send[off, pl.ds(r * chunk, chunk), :] = project(r, target).astype(BF16)
            pair_copy(off, r).start()

    send_half(offs[0])
    for n, off in enumerate(offs):
        for r in range(chunks):
            cut = pl.ds(r * chunk, chunk)
            value = project(r, tp_at(off))
            pair_copy(off, r).wait_recv()
            value = value + d_recv[off, cut, :].astype(F32)
            if off:
                y_send[off, cut, :] = value.astype(BF16)
                far_copy(off, r).start()
            else:
                acc[cut, pl.ds(0, depth)] = value
        if n + 1 < len(offs):
            send_half(offs[n + 1])
    for r in range(chunks):
        cut = pl.ds(r * chunk, chunk)
        value = acc[cut, pl.ds(0, depth)]
        for off in range(1, chips):
            far_copy(off, r).wait_recv()
            value = value + y_recv[off, cut, :].astype(F32)
        out[cut, :] = value.astype(BF16)

    near.wait_send()
    for copy in sends + forwards:
        copy.wait_send()

    def drain(s, carry):
        for h in range(heads):
            spread(me - s, h, lambda copy: copy.wait_send())
        return carry

    lax.fori_loop(0, me + 1, drain, 0)

    @pl.when(me + 1 < shards)
    def _():
        remote(st_out, st_in, st_s, st_r, me + 1, t).wait_send()

    for off in offs:
        for r in range(chunks):
            pair_copy(off, r).wait_send()
            if off:
                far_copy(off, r).wait_send()


def body(
    tokens,
    ret_query,
    ret_key,
    ret_value,
    stick_query,
    stick_key,
    stick_value,
    log_decay,
    stick_bias,
    out_ret,
    out_stick,
):
    shards, parts = lax.axis_size("sp"), lax.axis_size("tp")
    rows, depth = tokens.shape
    width = ret_query.shape[1]
    heads = width // HEAD_DIM
    chips = parts // CORES
    across = row_width(shards)
    chunk = 128 if rows % 128 == 0 else rows
    chunks = rows // chunk
    half = HEAD_DIM // 2
    inverse = np.float32(ROPE_BASE) ** (-np.arange(half, dtype=np.float32) / np.float32(half))
    inverse = jnp.asarray(np.tile(inverse, 2)[None, :], F32)
    any_spec = pl.BlockSpec(memory_space=pl.ANY)
    vmem = pl.BlockSpec(memory_space=pltpu.VMEM)
    dma = pltpu.SemaphoreType.DMA
    return pl.pallas_call(
        functools.partial(kernel, shards, parts),
        out_shape=jax.ShapeDtypeStruct((rows, depth), BF16),
        in_specs=[any_spec] * 9 + [vmem] * 2 + [pl.BlockSpec(memory_space=pltpu.SMEM)],
        out_specs=vmem,
        scratch_shapes=[
            pltpu.VMEM((parts, rows, depth), BF16),
            pltpu.VMEM((parts * depth, 6 * width), BF16),
            pltpu.VMEM((2 * width, parts * depth), BF16),
            pltpu.VMEM((rows, max(6 * width, heads * rows, depth)), F32),
            pltpu.VMEM((shards, heads, 2, rows, HEAD_DIM), BF16),
            pltpu.VMEM((rows, width), BF16),
            pltpu.VMEM((heads, rows, HEAD_DIM), BF16),
            pltpu.VMEM((rows, width), BF16),
            pltpu.VMEM((heads, rows, rows), F32),
            pltpu.VMEM((rows, rows), BF16),
            pltpu.VMEM((heads, rows, HEAD_DIM), F32),
            pltpu.VMEM((heads, HEAD_DIM, HEAD_DIM), F32),
            pltpu.VMEM((heads, HEAD_DIM, HEAD_DIM), BF16),
            pltpu.VMEM((heads, HEAD_DIM, HEAD_DIM), BF16),
            pltpu.VMEM((heads, rows, HEAD_DIM), F32),
            pltpu.VMEM((heads, rows, HEAD_DIM), F32),
            pltpu.VMEM((rows, 2 * width), BF16),
            pltpu.VMEM((2, rows, HEAD_DIM), F32),
            pltpu.VMEM((chips, rows, depth), BF16),
            pltpu.VMEM((chips, rows, depth), BF16),
            pltpu.VMEM((chips, rows, depth), BF16),
            pltpu.VMEM((chips, rows, depth), BF16),
            dma((8,)),
            dma,
            dma((chips,)),
            dma((chips,)),
            dma((chips,)),
            dma((chips,)),
            dma((shards, across, heads)),
            dma((shards, heads)),
            dma,
            dma,
            dma((chips, chunks)),
            dma((chips, chunks)),
            dma((chips, chunks)),
            dma((chips, chunks)),
        ],
        compiler_params=pltpu.CompilerParams(
            collective_id=0, has_side_effects=True, vmem_limit_bytes=60000 * 1024
        ),
    )(
        tokens,
        ret_query,
        ret_key,
        ret_value,
        stick_query,
        stick_key,
        stick_value,
        out_ret,
        out_stick,
        log_decay,
        inverse,
        stick_bias,
    )


def wide_kernel(
    shards,
    parts,
    tok,
    w_rq,
    w_rk,
    w_rv,
    w_sq,
    w_sk,
    w_sv,
    o_ret,
    o_stick,
    log_decay,
    inverse,
    bias,
    out,
    xs,
    wall,
    wo,
    kv,
    kv_out,
    q_all,
    q_out,
    q_far,
    far_run,
    far_past,
    far_out,
    far_in,
    ret_q,
    ret_k,
    ret_v,
    decay,
    tri,
    cumb,
    local,
    fresh_out,
    fresh_in,
    end_out,
    end_in,
    plane_out,
    plane_end,
    plane_in,
    ends_in,
    state_at,
    st_side,
    st_own,
    running,
    trailing,
    turn,
    f_ret,
    s_out,
    f_stick,
    acc,
    w_sem,
    wo_sem,
    tok_sem,
    own_s,
    own_r,
    fwd_s,
    fwd_r,
    kx_s,
    kx_r,
    kz_s,
    kz_r,
    q_s,
    q_r,
    qf_s,
    qf_r,
    fb_s,
    fb_r,
    fr_s,
    fr_r,
    en_s,
    en_r,
    sz_s,
    sz_r,
    se_s,
    se_r,
    sx_s,
    sx_r,
    wy_s,
    wx_s,
    ww_r,
    rf_s,
    rf_r,
    rp_s,
    rp_r,
    fd_s,
    fd_r,
    fp_s,
    fp_r,
):
    rows, depth = tok.shape
    width = w_rq.shape[1]
    heads = width // HEAD_DIM
    chips = parts // CORES
    across = row_width(shards)
    planes = shards // across
    me = lax.axis_index("sp")
    t = lax.axis_index("tp")
    chip = t // CORES
    core = t % CORES
    partner = chip * CORES + (1 - core)
    x = me % across
    z = me // across
    first = me - x
    chunk = CHUNK
    chunks = rows // chunk
    bit = BIT
    bits = rows // bit
    plane_rows = across * rows
    tiles = plane_rows // TILE
    scale = HEAD_DIM ** (-0.5)
    last = planes - 1

    def chip_at(off):
        return lax.rem(chip + off, chips)

    def tp_at(off):
        return chip_at(off) * CORES + core

    def col_at(off):
        return lax.rem(x + off, across)

    def cut_of(c):
        return pl.ds(c * chunk, chunk)

    def bit_of(c):
        return pl.ds(c * bit, bit)

    def remote(src, dst, send, recv, sp_index, tp_index):
        return pltpu.make_async_remote_copy(
            src_ref=src,
            dst_ref=dst,
            send_sem=send,
            recv_sem=recv,
            device_id={"sp": sp_index, "tp": tp_index},
            device_id_type=pl.DeviceIdType.MESH,
        )

    own_load = pltpu.make_async_copy(tok, xs.at[t], tok_sem)
    own_load.start()

    barrier = pltpu.get_barrier_semaphore()

    def greet(sp_index, tp_index):
        pl.semaphore_signal(
            barrier,
            inc=1,
            device_id={"sp": sp_index, "tp": tp_index},
            device_id_type=pl.DeviceIdType.MESH,
        )

    for off in range(1, parts):
        greet(me, lax.rem(t + off, parts))
    for off in range(1, shards):
        greet(lax.rem(me + off, shards), t)
    for joff in range(1, across):
        for off in range(1, chips):
            greet(first + col_at(joff), tp_at(off))
    count = (parts - 1) + (shards - 1) + (across - 1) * (chips - 1)
    up = z < last
    down = z > 0
    upper = z >= 2
    lower = z + 2 < planes
    own_load.wait()
    for i, w in enumerate((w_sk, w_sv, w_sq, w_rk, w_rv, w_rq)):
        pltpu.make_async_copy(w, wall.at[:, pl.ds(i * width, width)], w_sem.at[i // 2]).start()

    def weights_in(i):
        at = wall.at[:, pl.ds(2 * i * width, 2 * width)]
        pltpu.make_async_copy(at, at, w_sem.at[i]).wait()

    pl.semaphore_wait(barrier, count)

    def token_copy(off, c):
        at = xs.at[t, bit_of(c), :]
        target = tp_at(off) if off else partner
        return remote(at, at, own_s.at[off], own_r.at[off, c], me, target)

    def token_forward(off, c):
        at = xs.at[tp_at(-off + chips), bit_of(c), :]
        return remote(at, at, fwd_s.at[off], fwd_r.at[off, c], me, partner)

    for c in range(bits):
        for off in tuple(range(1, chips)) + (0,):
            token_copy(off, c).start()

    mixers = (o_ret, o_stick)
    def near_weight(m):
        return remote(
            mixers[m].at[:, pl.ds(pl.multiple_of(partner * depth, depth), depth)],
            wo.at[m, pl.ds(pl.multiple_of(t * width, width), width), :],
            wy_s,
            ww_r.at[2],
            me,
            partner,
        )

    blocks = (width // 2, width // across)
    mine = (z % 2, x)

    def share_at(m, s):
        lo = s * width + mine[m] * blocks[m]
        return pl.ds(pl.multiple_of(lo, HEAD_DIM), blocks[m])

    def far_weight(m, off, k):
        j = chip_at(off) * CORES + k
        return remote(
            mixers[m].at[
                pl.ds(pl.multiple_of(mine[m] * blocks[m], HEAD_DIM), blocks[m]),
                pl.ds(pl.multiple_of(j * depth, depth), depth),
            ],
            wo.at[m, share_at(m, t), :],
            wy_s,
            ww_r.at[m],
            me,
            j,
        )

    def side_weight(m, s, off):
        at = wo.at[m, share_at(m, s), :]
        target = first + col_at(off) if m else me + across * (1 - 2 * mine[0])
        return remote(at, at, wx_s.at[m], ww_r.at[3 + m], target, t)

    def arrival(at, sem):
        pltpu.make_async_copy(at, at, sem).wait()

    far_tp = [
        chip_at(off) * CORES + k for off in range(1, chips) for k in range(CORES)
    ]

    sides = (1, across - 1)

    def side_rows(m):
        return pl.ds(0, len(far_tp) * sides[m] * blocks[m])

    def relay_weights(m):
        arrival(wo.at[0, pl.ds(0, len(far_tp) * blocks[m]), :], ww_r.at[m])
        for s in far_tp:
            for off in range(1, sides[m] + 1):
                side_weight(m, s, off).start()

    for m in range(2):
        for off in range(1, chips):
            for k in range(CORES):
                far_weight(m, off, k).start()
        near_weight(m).start()
    own_out = []
    for m in range(2):
        load = pltpu.make_async_copy(
            mixers[m].at[:, pl.ds(pl.multiple_of(t * depth, depth), depth)],
            wo.at[m, pl.ds(pl.multiple_of(t * width, width), width), :],
            wo_sem.at[m],
        )
        load.start()
        own_out.append(load)

    lane = lax.broadcasted_iota(jnp.int32, (rows, rows), 1)
    sub = lax.broadcasted_iota(jnp.int32, (rows, rows), 0)
    for h in range(heads):
        ld_row = jnp.broadcast_to(log_decay[h : h + 1, :], (rows, rows))
        cum_col = jnp.sum(jnp.where(lane <= sub, ld_row, 0.0), axis=1, keepdims=True)
        ld_col = jnp.sum(jnp.where(sub == lane, ld_row, 0.0), axis=1, keepdims=True)
        cum_row = jnp.sum(
            jnp.where(sub <= lane, jnp.broadcast_to(ld_col, (rows, rows)), 0.0),
            axis=0,
            keepdims=True,
        )
        gaps = cum_col - cum_row
        decay[h] = jnp.where(lane <= sub, jnp.exp(jnp.where(lane <= sub, gaps, 0.0)), 0.0)
        cumb[h] = jnp.broadcast_to(cum_col, (rows, HEAD_DIM))
    tri[...] = (
        lax.broadcasted_iota(jnp.int32, (TILE, TILE), 0)
        > lax.broadcasted_iota(jnp.int32, (TILE, TILE), 1)
    ).astype(BF16)

    angles = (
        me * rows + lax.broadcasted_iota(jnp.int32, (rows, HEAD_DIM), 0)
    ).astype(F32) * inverse[...]
    left = lax.broadcasted_iota(jnp.int32, (rows, HEAD_DIM), 1) < HEAD_DIM // 2
    sine = jnp.sin(angles)
    turn[0] = jnp.cos(angles)
    turn[1] = jnp.where(left, -sine, sine)

    def weight(j, lo, size):
        return wall[pl.ds(pl.multiple_of(j * depth, depth), depth), pl.ds(lo, size)]

    def plane_cut(j, c):
        return pl.ds(pl.multiple_of(j * rows + c * chunk, chunk), chunk)

    def plane_bit(j, c):
        return pl.ds(pl.multiple_of(j * rows + c * bit, bit), bit)

    def plane_rows_of(j):
        return pl.ds(pl.multiple_of(j * rows, rows), rows)

    def kx_copy(off, c, col):
        j = col_at(off)
        return remote(
            kv_out.at[j, :, bit_of(c), :],
            kv.at[0, :, plane_bit(col, c), :],
            kx_s.at[off],
            kx_r.at[col, c],
            first + j,
            t,
        )

    def kz_copy(j, c):
        return remote(
            kv.at[0, :, plane_bit(j, c), :],
            kv.at[1, :, plane_bit(j, c), :],
            kz_s,
            kz_r,
            me + across,
            t,
        )

    def relay_x(c):
        for off in range(1, across):
            kx_copy(off, c, col_at(off)).wait_recv()

            @pl.when(up)
            def _():
                kz_copy(col_at(off), c).start()

    def q_copy(off, c, col):
        j = col_at(off)
        return remote(
            q_out.at[j, cut_of(c), :],
            q_all.at[plane_cut(col, c), :],
            q_s.at[off],
            q_r.at[col],
            first + j,
            t,
        )

    def far_q(off, c, col):
        j = col_at(off)
        return remote(
            q_out.at[j, cut_of(c), :],
            q_far.at[plane_cut(col, c), :],
            qf_s,
            qf_r,
            first - 2 * across + j,
            t,
        )

    def far_back(r):
        at = pl.ds(r * TILE, TILE)
        return remote(
            far_out.at[at, :], far_in.at[at, :], fb_s, fb_r.at[r], me + 2 * across, t
        )

    def turned(u, cut):
        return u * turn[0, cut, :] + pltpu.roll(u, HEAD_DIM // 2, 1) * turn[1, cut, :]

    def projected(lo, size, cut):
        value = dot(xs[sources[0], cut, :], weight(sources[0], lo, size))
        for j in sources[1:]:
            value = value + dot(xs[j, cut, :], weight(j, lo, size))
        return value

    def project_q(c):
        cut = cut_of(c)
        value = (projected(2 * width, width, cut) * (scale * LOG2E)).astype(BF16)
        for h in range(heads):
            q_out[h, cut, :] = value[:, h * HEAD_DIM : (h + 1) * HEAD_DIM]

        @pl.when(upper)
        def _():
            for off in range(across - 1, -1, -1):
                far_q(off, c, x).start()

        for off in range(1, across):
            q_copy(off, c, x).start()
        q_all[plane_cut(x, c), :] = q_out[x, cut, :]

    def project_kv(c):
        cut = cut_of(c)
        value = projected(3 * width, 2 * width, cut).astype(BF16)
        for h in range(heads):
            lo = h * HEAD_DIM
            ret_k[h, cut, :] = (
                turned(value[:, lo : lo + HEAD_DIM].astype(F32), cut) * scale
            ).astype(BF16)
            ret_v[h, cut, :] = value[:, width + lo : width + lo + HEAD_DIM]

    def project_rq(c):
        cut = cut_of(c)
        value = projected(5 * width, width, cut).astype(BF16).astype(F32)
        for h in range(heads):
            ret_q[h, cut, :] = turned(value[:, h * HEAD_DIM : (h + 1) * HEAD_DIM], cut).astype(
                BF16
            )

    def relay_down(*items):
        @pl.when(down)
        def _():
            for off, c in items:
                relay_z(z - 1, col_at(off), c)

    weights_in(0)
    far_same = [tp_at(-off + chips) for off in range(1, chips)]
    far_other = [chip_at(-off + chips) * CORES + (1 - core) for off in range(1, chips)]
    sources = [t, partner] + far_same + far_other
    per_chunk = chunk // bit
    for c in range(bits):
        cut = bit_of(c)
        token_copy(0, c).wait_recv()
        value = dot(xs[t, cut, :], weight(t, 0, 2 * width))
        value = value + dot(xs[partner, cut, :], weight(partner, 0, 2 * width))
        for off in range(1, chips):
            token_copy(off, c).wait_recv()
            token_forward(off, c).start()
            j = far_same[off - 1]
            value = value + dot(xs[j, cut, :], weight(j, 0, 2 * width))
        if c >= 3:
            relay_x(c - 3)
        if c == 2:
            weights_in(1)
            weights_in(2)
        group, side = (c - per_chunk) // per_chunk, (c - per_chunk) % per_chunk
        if group >= 0:
            if side == 0:
                project_q(group)
                project_rq(group)
            if side == per_chunk - 1:
                project_kv(group)
        for off in range(1, chips):
            token_forward(off, c).wait_recv()
            j = far_other[off - 1]
            value = value + dot(xs[j, cut, :], weight(j, 0, 2 * width))
        value = value.astype(BF16)
        for i in range(2):
            for h in range(heads):
                lo = i * width + h * HEAD_DIM
                kv_out[h, i, cut, :] = value[:, lo : lo + HEAD_DIM]

        for off in range(1, across):
            kx_copy(off, c, x).start()
        for i in range(2):
            kv[0, i, plane_bit(x, c), :] = kv_out[x, i, cut, :]

        @pl.when(up)
        def _():
            kz_copy(x, c).start()


    project_q(chunks - 1)
    relay_x(bits - 3)
    project_kv(chunks - 1)
    for h in range(heads):
        cum = cumb[h]
        end = cum[rows - 1 : rows, :]
        weighted = (ret_k[h].astype(F32) * jnp.exp(end - cum)).astype(BF16)
        fresh_out[h] = dot(weighted.T, ret_v[h]).astype(BF16)
        end_out[h] = jnp.broadcast_to(jnp.exp(end), (8, HEAD_DIM))

    def fresh_copy(off, col):
        j = col_at(off)
        return remote(
            fresh_out.at[j], fresh_in.at[col], fr_s.at[off], fr_r.at[col], first + j, t
        )

    def end_copy(off, col):
        j = col_at(off)
        return remote(end_out.at[j], end_in.at[col], en_s.at[off], en_r.at[col], first + j, t)

    for off in range(1, across):
        fresh_copy(off, x).start()
        end_copy(off, x).start()

    relay_x(bits - 2)
    project_rq(chunks - 1)
    relay_x(bits - 1)
    for h in range(heads):
        scores = (nt(ret_q[h], ret_k[h]) * decay[h]).astype(BF16)
        local[h] = dot(scores, ret_v[h])
    running[...] = jnp.zeros_like(running)
    trailing[...] = jnp.zeros_like(trailing)
    shift = bias[x] * LOG2E

    def stick(r, p, b, diagonal, query=q_all, total=running, past=trailing):
        at_r = pl.ds(r * TILE, TILE)
        at_b = pl.ds(pl.multiple_of(b * TILE, TILE), TILE)
        logits = nt(query[at_r, :], kv[p, 0, at_b, :]) + shift
        soft = jnp.maximum(
            logits, jnp.log(1.0 + jnp.exp2(jnp.minimum(logits, CLIP))) * LOG2E
        )
        taken = logits - soft
        if diagonal:
            seen = lax.broadcasted_iota(jnp.int32, (TILE, TILE), 1) < lax.broadcasted_iota(
                jnp.int32, (TILE, TILE), 0
            )
            soft = jnp.where(seen, soft, 0.0)
        suffix = dot(soft.astype(BF16), tri[...])
        weights = jnp.exp2(taken - suffix)
        if diagonal:
            weights = jnp.where(seen, weights, 0.0)
        partial = dot(weights.astype(BF16), kv[p, 1, at_b, :])
        behind = past[at_r, :]
        total[at_r, :] += jnp.exp2(-behind) * partial
        past[at_r, :] = behind + jnp.broadcast_to(
            suffix[:, 0:1] + soft[:, 0:1], (TILE, HEAD_DIM)
        )

    def summary(p, target):
        return remote(
            plane_out, plane_in.at[p], sz_s.at[target], sz_r.at[p], target * across + x, t
        )

    def summary_end(p, target):
        return remote(
            plane_end, ends_in.at[p], se_s.at[target], se_r.at[p], target * across + x, t
        )

    for off in range(1, across):
        j = col_at(off)
        arrival(q_all.at[plane_rows_of(j), :], q_r.at[j])
    for r in range(tiles):
        for b in range(r, -1, -1):
            stick(r, 0, b, b == r)
    fresh_in[x] = fresh_out[x]
    end_in[x] = end_out[x]
    for off in range(1, across):
        j = col_at(off)
        fresh_copy(off, j).wait_recv()
        end_copy(off, j).wait_recv()
    value = fresh_in[0].astype(F32)
    scales = end_in[0]
    for j in range(1, across):
        value = end_in[j, 0:1, :] * value + fresh_in[j].astype(F32)
        scales = scales * end_in[j]
    plane_out[...] = value.astype(BF16)
    plane_end[...] = scales
    for target in range(1, planes):

        @pl.when(target > z)
        def _():
            summary(z, target).start()
            summary_end(z, target).start()

    def state_side(off, col):
        j = col_at(off)
        return remote(st_side.at[j], st_own.at[col], sx_s.at[off], sx_r.at[col], first + j, t)

    def advance():
        state_at[...] = jnp.zeros_like(state_at)
        for p in range(planes - 1):

            @pl.when(p < z)
            def _():
                summary(p, 0).wait_recv()
                summary_end(p, 0).wait_recv()
                state_at[...] = ends_in[p, 0:1, :] * state_at[...] + plane_in[p].astype(F32)

        state = state_at[...]
        for j in range(across):
            st_side[j] = state.astype(BF16)
            state = end_in[j, 0:1, :] * state + fresh_in[j].astype(F32)
        st_own[x] = st_side[x]
        for off in range(1, across):
            state_side(off, x).start()


    @pl.when(z == 0)
    def _():
        advance()

    relay_weights(0)

    @pl.when(down)
    def _():
        arrival(kv.at[1], kz_r)

    def ret_copy(off):
        at = f_ret.at[t]
        target = tp_at(off) if off else partner
        return remote(at, at, rf_s.at[off], rf_r.at[off], me, target)

    def finish_ret():
        for off in range(1, across):
            state_side(off, col_at(off)).wait_recv()
        for h in range(heads):
            carried = dot(ret_q[h], st_own[h]) * jnp.exp(cumb[h])
            f_ret[t, :, pl.ds(h * HEAD_DIM, HEAD_DIM)] = head_norm(local[h] + carried).astype(
                BF16
            )
        for off in range(chips):
            ret_copy(off).start()


    @pl.when(z == 0)
    def _():
        relay_weights(1)


    @pl.when(lower)
    def _():
        arrival(q_far, qf_r)
        far_run[...] = jnp.zeros_like(far_run)
        far_past[...] = jnp.zeros_like(far_past)
        for lo in range(0, tiles, 2):
            group = range(lo, min(lo + 2, tiles))
            for b in range(tiles - 1, -1, -1):
                for r in group:
                    stick(r, 0, b, False, q_far, far_run, far_past)

            @pl.when(down)
            def _():
                for b in range(tiles - 1, -1, -1):
                    for r in group:
                        stick(r, 1, b, False, q_far, far_run, far_past)

            for r in group:
                at = pl.ds(r * TILE, TILE)
                far_out[at, :] = far_run[at, :].astype(BF16)
                far_back(r).start()
            if lo == 0:

                @pl.when(down)
                def _():
                    advance()

        @pl.when(down)
        def _():
            relay_weights(1)

        finish_ret()

    def ret_forward(off):
        at = f_ret.at[tp_at(-off + chips)]
        return remote(at, at, rp_s.at[off], rp_r.at[off], me, partner)

    def visit(p, b):
        for r in range(tiles):
            stick(r, p, b, False)


    @pl.when(down)
    def _():
        for b in range(tiles - 1, -1, -1):
            visit(1, b)


    @pl.when(upper)
    def _():
        advance()
        relay_weights(1)
        finish_ret()


    def direct_copy(off, j, c):
        return remote(
            s_out.at[j, cut_of(c), :],
            f_stick.at[t, x, cut_of(c), :],
            fd_s.at[off],
            fd_r.at[chip, x, c],
            first + j,
            tp_at(off),
        )

    def pair_copy(off, j, c):
        at = f_stick.at[chip_at(off) * CORES + core, j, cut_of(c), :]
        return remote(at, at, fp_s, fp_r.at[c], me, partner)

    for n in range(across * chunks):
        j, c = n // chunks, n % chunks
        if (n * chunk) % TILE == 0:
            r = n * chunk // TILE

            @pl.when(upper)
            def _():
                far_back(r).wait_recv()
                at = pl.ds(r * TILE, TILE)
                running[at, :] += jnp.exp2(-trailing[at, :]) * far_in[at, :].astype(F32)

        value = head_norm(running[pl.ds(n * chunk, chunk), :]).astype(BF16)
        s_out[j, cut_of(c), :] = value
        for off in range(chips - 1, 0, -1):
            direct_copy(off, j, c).start()

        @pl.when(j == x)
        def _():
            f_stick[t, x, cut_of(c), :] = s_out[j, cut_of(c), :]
            pair_copy(0, x, c).start()

        @pl.when(j != x)
        def _():
            direct_copy(0, j, c).start()

    for off in range(1, chips):
        ret_copy(off).wait_recv()
        ret_forward(off).start()

    def direct_in(c):
        for joff in range(across - 1, -1, -1):
            for off in range(chips):
                if off or joff:
                    k, j = chip_at(off), col_at(joff)
                    arrival(f_stick.at[k * CORES + core, j, cut_of(c), :], fd_r.at[k, j, c])
                    pair_copy(off, j, c).start()

    for c in range(chunks - 1):
        direct_in(c)
    ret_copy(0).wait_recv()
    for load in own_out:
        load.wait()
    arrival(wo.at[0, pl.ds(0, 2 * width), :], ww_r.at[2])
    arrival(wo.at[0, side_rows(0), :], ww_r.at[3])
    for off in range(1, chips):
        ret_forward(off).wait_recv()
    features = jnp.concatenate([f_ret[s] for s in range(parts)], axis=1)
    acc[...] = dot(features, wo[0])
    direct_in(chunks - 1)
    arrival(wo.at[1, side_rows(1), :], ww_r.at[4])
    for c in range(chunks):
        cut = cut_of(c)
        arrival(f_stick.at[pl.ds(0, chips), :, cut, :], fp_r.at[c])
        features = jnp.concatenate(
            [f_stick[s, j, cut, :] for s in range(parts) for j in range(across)], axis=1
        )
        out[cut, :] = (acc[cut, :] + dot(features, wo[1])).astype(BF16)
    for off in range(chips):
        arrival(xs.at[0], own_s.at[off])
        if off:
            arrival(xs.at[0], fwd_s.at[off])
            arrival(f_stick.at[0], fd_s.at[off])
        ret_copy(off).wait_send()
        if off:
            ret_forward(off).wait_send()
    arrival(f_stick.at[0, pl.ds(0, across - 1)], fd_s.at[0])
    arrival(f_stick.at[pl.ds(0, chips)], fp_s)
    sent = 2 * width + len(far_tp) * (blocks[0] + blocks[1])
    arrival(wo.at[0, pl.ds(0, sent), :], wy_s)
    for m in range(2):
        arrival(wo.at[m, side_rows(m), :], wx_s.at[m])
    for off in range(1, across):
        arrival(kv_out.at[0], kx_s.at[off])
        arrival(q_out.at[0], q_s.at[off])
        fresh_copy(off, x).wait_send()
        end_copy(off, x).wait_send()
        state_side(off, x).wait_send()
    for target in range(1, planes):

        @pl.when(target > z)
        def _():
            summary(z, target).wait_send()
            summary_end(z, target).wait_send()

    @pl.when(up)
    def _():
        arrival(kv.at[0], kz_s)

    @pl.when(lower)
    def _():
        arrival(far_out, fb_s)

    @pl.when(upper)
    def _():
        arrival(q_out, qf_s)


def wide_body(
    tokens,
    ret_query,
    ret_key,
    ret_value,
    stick_query,
    stick_key,
    stick_value,
    log_decay,
    stick_bias,
    out_ret,
    out_stick,
):
    shards, parts = lax.axis_size("sp"), lax.axis_size("tp")
    rows, depth = tokens.shape
    width = ret_query.shape[1]
    heads = width // HEAD_DIM
    chips = parts // CORES
    across = row_width(shards)
    planes = shards // across
    chunks = rows // CHUNK
    bits = rows // BIT
    plane_rows = across * rows
    half = HEAD_DIM // 2
    inverse = np.float32(ROPE_BASE) ** (-np.arange(half, dtype=np.float32) / np.float32(half))
    inverse = jnp.asarray(np.tile(inverse, 2)[None, :], F32)
    any_spec = pl.BlockSpec(memory_space=pl.ANY)
    vmem = pl.BlockSpec(memory_space=pltpu.VMEM)
    dma = pltpu.SemaphoreType.DMA
    square = (HEAD_DIM, HEAD_DIM)
    return pl.pallas_call(
        functools.partial(wide_kernel, shards, parts),
        out_shape=jax.ShapeDtypeStruct((rows, depth), BF16),
        in_specs=[any_spec] * 9 + [vmem] * 2 + [pl.BlockSpec(memory_space=pltpu.SMEM)],
        out_specs=vmem,
        scratch_shapes=[
            pltpu.VMEM((parts, rows, depth), BF16),
            pltpu.VMEM((parts * depth, 6 * width), BF16),
            pltpu.VMEM((2, parts * width, depth), BF16),
            pltpu.VMEM((2, 2, plane_rows, HEAD_DIM), BF16),
            pltpu.VMEM((across, 2, rows, HEAD_DIM), BF16),
            pltpu.VMEM((plane_rows, HEAD_DIM), BF16),
            pltpu.VMEM((across, rows, HEAD_DIM), BF16),
            pltpu.VMEM((plane_rows, HEAD_DIM), BF16),
            pltpu.VMEM((plane_rows, HEAD_DIM), F32),
            pltpu.VMEM((plane_rows, HEAD_DIM), F32),
            pltpu.VMEM((plane_rows, HEAD_DIM), BF16),
            pltpu.VMEM((plane_rows, HEAD_DIM), BF16),
            pltpu.VMEM((heads, rows, HEAD_DIM), BF16),
            pltpu.VMEM((heads, rows, HEAD_DIM), BF16),
            pltpu.VMEM((heads, rows, HEAD_DIM), BF16),
            pltpu.VMEM((heads, rows, rows), F32),
            pltpu.VMEM((TILE, TILE), BF16),
            pltpu.VMEM((heads, rows, HEAD_DIM), F32),
            pltpu.VMEM((heads, rows, HEAD_DIM), F32),
            pltpu.VMEM((heads,) + square, BF16),
            pltpu.VMEM((across,) + square, BF16),
            pltpu.VMEM((heads, 8, HEAD_DIM), F32),
            pltpu.VMEM((across, 8, HEAD_DIM), F32),
            pltpu.VMEM(square, BF16),
            pltpu.VMEM((8, HEAD_DIM), F32),
            pltpu.VMEM((planes,) + square, BF16),
            pltpu.VMEM((planes, 8, HEAD_DIM), F32),
            pltpu.VMEM(square, F32),
            pltpu.VMEM((across,) + square, BF16),
            pltpu.VMEM((across,) + square, BF16),
            pltpu.VMEM((plane_rows, HEAD_DIM), F32),
            pltpu.VMEM((plane_rows, HEAD_DIM), F32),
            pltpu.VMEM((2, rows, HEAD_DIM), F32),
            pltpu.VMEM((parts, rows, width), BF16),
            pltpu.VMEM((across, rows, HEAD_DIM), BF16),
            pltpu.VMEM((parts, across, rows, HEAD_DIM), BF16),
            pltpu.VMEM((rows, depth), F32),
            dma((3,)),
            dma((2,)),
            dma,
            dma((chips,)),
            dma((chips, bits)),
            dma((chips,)),
            dma((chips, bits)),
            dma((across,)),
            dma((across, bits)),
            dma,
            dma,
            dma((across,)),
            dma((across,)),
            dma,
            dma,
            dma,
            dma((plane_rows // TILE,)),
            dma((across,)),
            dma((across,)),
            dma((across,)),
            dma((across,)),
            dma((planes,)),
            dma((planes,)),
            dma((planes,)),
            dma((planes,)),
            dma((across,)),
            dma((across,)),
            dma,
            dma((2,)),
            dma((5,)),
            dma((chips,)),
            dma((chips,)),
            dma((chips,)),
            dma((chips,)),
            dma((chips,)),
            dma((chips, across, chunks)),
            dma,
            dma((chunks,)),
        ],
        compiler_params=pltpu.CompilerParams(
            collective_id=0, has_side_effects=True, vmem_limit_bytes=60000 * 1024
        ),
    )(
        tokens,
        ret_query,
        ret_key,
        ret_value,
        stick_query,
        stick_key,
        stick_value,
        out_ret,
        out_stick,
        log_decay.T,
        inverse,
        stick_bias,
    )


def pick(tokens, ret_query, *rest):
    shards = lax.axis_size("sp")
    rows, heads = tokens.shape[0], ret_query.shape[1] // HEAD_DIM
    across = row_width(shards)
    wide = heads == across and rows % CHUNK == 0 and (across * rows) % TILE == 0 and shards == 4 * across
    return (wide_body if wide else body)(tokens, ret_query, *rest)


def solution(mesh):
    in_specs = (
        P("sp", "tp"),
        P(None, "tp"),
        P(None, "tp"),
        P(None, "tp"),
        P(None, "tp"),
        P(None, "tp"),
        P(None, "tp"),
        P("sp", "tp"),
        P("tp"),
        P("tp", None),
        P("tp", None),
    )
    return jax.shard_map(
        pick, mesh=mesh, in_specs=in_specs, out_specs=P("sp", "tp"), check_vma=False
    )
```
